256 devices in a mesh: sp: 32 (over z, y), tp: 8 (over x, core).
Axes of the slice: x: 4, y: 4, z: 8, core: 2. Of those that a mesh axis runs over, the one named last changes fastest.
Arguments:
- queries: bfloat16 [16384, 1024], P('sp', 'tp'), may hold values from -6 to 6
- keys: bfloat16 [16384, 1024], P('sp', 'tp'), may hold values from -6 to 6
- values: bfloat16 [16384, 1024], P('sp', 'tp'), may hold values from -12 to 12
- breaks: bfloat16 [16384, 8], P('sp', 'tp'), may hold values from -12 to 0.5
- residual_in: bfloat16 [16384, 2048], P('sp', 'tp'), may hold values from -6 to 6
- out_weight: bfloat16 [1024, 2048], P('tp'), may hold values from -0.1875 to 0.1875
- first_gain: float32 [2048], replicated, may hold values from 0.1 to 1.9
- first_shift: float32 [2048], replicated, may hold values from -2 to 2
- up_weight: bfloat16 [2048, 8192], P('sp', 'tp'), may hold values from -0.125 to 0.125
- down_weight: bfloat16 [2048, 8192], P('sp', 'tp'), may hold values from -0.0625 to 0.0625
- second_gain: float32 [2048], replicated, may hold values from 0.1 to 1.9
- second_shift: float32 [2048], replicated, may hold values from -2 to 2
Outputs:
- layer_out: bfloat16 [16384, 2048], P('sp', 'tp')
The draws below stay inside these ranges and needn't reach their ends.
All inputs are finite; a program needn't handle non-finite values.
Results may differ from the reference program's by a relative error of at most 0.018.
Values may be sent and summed in bfloat16 or wider, within the bound.
A program may use at most 128 MiB of HBM per device.

```python
import math
import jax
import jax.numpy as jnp
from jax import lax

D = 2048
FF = 8192
HEAD_COUNT = 8
HD = 128
KEY_BLOCK = 512
TOK_DEV = 512
SEQUENCE_LENGTH = 16384
N_TP = 8


def draw_values(key, part):
    offset_key, noise_key = jax.random.split(jax.random.fold_in(key, 29), 2)
    offset = jax.random.normal(offset_key, (HEAD_COUNT * HD,), jnp.float32) * 1.5
    noise = jax.random.normal(noise_key, (SEQUENCE_LENGTH, HEAD_COUNT * HD), jnp.float32) * 2.0
    return jnp.clip(noise + offset[None, :], -12.0, 12.0).astype(jnp.bfloat16)


def draw_breaks(key, part):
    gradual_key, quick_key, key_tile_rows, noise_key, spike_key, height_key = jax.random.split(jax.random.fold_in(key, 17), 6)
    slow_share = 0.5
    slow_heads = jax.random.uniform(gradual_key, (HEAD_COUNT,)) < slow_share
    slow_base = math.log(1.0 / SEQUENCE_LENGTH) - 0.5
    fast_base = -4.2 + jax.random.uniform(quick_key, (HEAD_COUNT,), minval=-0.3, maxval=0.3)
    head_base = jnp.where(slow_heads, slow_base, fast_base)
    by_block = jax.random.uniform(key_tile_rows, (SEQUENCE_LENGTH // TOK_DEV, HEAD_COUNT), minval=0.0, maxval=math.log(2.5))
    blockwise = jnp.repeat(by_block, TOK_DEV, axis=0)
    jitter = jax.random.uniform(noise_key, (SEQUENCE_LENGTH, HEAD_COUNT), minval=-0.35, maxval=0.35)
    height_values = head_base[None, :] + blockwise + jitter
    spiky_scores = jax.random.uniform(spike_key, (SEQUENCE_LENGTH, HEAD_COUNT)) < 4.0 / SEQUENCE_LENGTH
    spike_height = jax.random.uniform(height_key, (SEQUENCE_LENGTH, HEAD_COUNT), minval=-1.5, maxval=0.0)
    return jnp.where(spiky_scores, spike_height, height_values).astype(jnp.bfloat16)


def block_scale(rng, shape, cuts, least, high):
    level = 1.0
    for dim, parts in cuts:
        heights = jax.random.uniform(jax.random.fold_in(jax.random.fold_in(rng, 6), dim), (parts,), jnp.float32, least / len(cuts), high / len(cuts))
        level = level * jnp.repeat(jnp.exp(heights), shape[dim] // parts).reshape((-1,) + (1,) * (len(shape) - 1 - dim))
    return level


def scatter_about(own_key, extent, width, limit, cuts=(), kind=jnp.bfloat16):
    factor_of = block_scale(own_key, extent, cuts, -0.22, 0.18) if cuts else 1.0
    drawn = jax.random.normal(own_key, extent, jnp.float32) * width * factor_of
    return jnp.minimum(jnp.maximum(drawn, -limit), limit).astype(kind)


def setup_inputs(seed: int = 0) -> dict:
    seeds = jax.random.split(jax.random.key(seed), 13)
    queries = scatter_about(seeds[0], (SEQUENCE_LENGTH, HEAD_COUNT * HD), 1.0, 6.0, ((0, 32), (1, 8)))
    keys = scatter_about(seeds[1], (SEQUENCE_LENGTH, HEAD_COUNT * HD), 1.0, 6.0, ((0, 32), (1, 8)))
    values = draw_values(jax.random.fold_in(seeds[12], 71), 0)
    breaks = draw_breaks(jax.random.fold_in(seeds[12], 71), 0)
    residual_in = scatter_about(seeds[4], (SEQUENCE_LENGTH, D), 1.0, 6.0, ((0, 32), (1, 8)))
    out_weight = scatter_about(seeds[5], (HEAD_COUNT * HD, D), (HEAD_COUNT * HD) ** -0.5, 0.1875, ((0, 8),))
    first_gain = jnp.clip(1.0 + 0.18 * jax.random.normal(seeds[6], (D,), jnp.float32), 0.1, 1.9)
    first_shift = scatter_about(seeds[7], (D,), 0.3, 2.0, (), jnp.float32)
    up_weight = scatter_about(seeds[8], (D, FF), D ** -0.5, 0.125, ((0, 32), (1, 8)))
    down_weight = scatter_about(seeds[9], (D, FF), FF ** -0.5, 0.0625, ((0, 32), (1, 8)))
    second_gain = jnp.clip(1.0 + 0.18 * jax.random.normal(seeds[10], (D,), jnp.float32), 0.1, 1.9)
    second_shift = scatter_about(seeds[11], (D,), 0.3, 2.0, (), jnp.float32)
    return dict(queries=queries, keys=keys, values=values, breaks=breaks, residual_in=residual_in, out_weight=out_weight, first_gain=first_gain, first_shift=first_shift, up_weight=up_weight, down_weight=down_weight, second_gain=second_gain, second_shift=second_shift)


ALPHA = 2.0 ** 0.25
EPSILON = 1e-05

def rounded(partial_value):
    return lax.optimization_barrier(partial_value.astype(jnp.bfloat16)).astype(jnp.float32)

def layer_norm(pre, gain, shift):
    center = lax.optimization_barrier(jnp.mean(pre, axis=-1, keepdims=True))
    centered = pre - center
    spread = lax.optimization_barrier(jnp.mean(centered * centered, axis=-1, keepdims=True))
    return centered * lax.rsqrt(spread + EPSILON) * gain + shift

def reference(queries, keys, values, breaks, residual_in, out_weight, first_gain, first_shift, up_weight, down_weight, second_gain, second_shift):
    query_heads = queries.reshape(SEQUENCE_LENGTH, HEAD_COUNT, HD).astype(jnp.float32)
    key_heads = keys.reshape(SEQUENCE_LENGTH, HEAD_COUNT, HD).astype(jnp.float32)
    value_heads = values.reshape(SEQUENCE_LENGTH, HEAD_COUNT, HD).astype(jnp.float32)
    break_rows = breaks.astype(jnp.float32).T
    positions = jnp.arange(SEQUENCE_LENGTH, dtype=jnp.int32)
    scale = HD ** (-0.5)

    def attend_block(index):
        first = index * KEY_BLOCK
        query_block = lax.dynamic_slice_in_dim(query_heads, first, KEY_BLOCK, 0)
        query_pos = first + jnp.arange(KEY_BLOCK, dtype=jnp.int32)
        scores = jnp.einsum('qhd,khd->hqk', query_block, key_heads) * scale + break_rows[:, None, :]
        strict = (positions[None, :] < query_pos[:, None])[None]
        log_break = jax.nn.log_sigmoid(scores)
        log_keep = jnp.where(strict, log_break - scores, 0.0)
        later = lax.cumsum(log_keep, axis=2, reverse=True) - log_keep
        weights = jnp.where(strict, jnp.exp(log_break + later), 0.0).astype(jnp.bfloat16)
        mixed_heads = jnp.einsum('hqk,khd->qhd', weights.astype(jnp.float32), value_heads)
        return mixed_heads.reshape(KEY_BLOCK, HEAD_COUNT * HD).astype(jnp.bfloat16)
    attended = lax.map(attend_block, jnp.arange(SEQUENCE_LENGTH // KEY_BLOCK, dtype=jnp.int32)).reshape(SEQUENCE_LENGTH, HEAD_COUNT * HD)
    group_width = HEAD_COUNT * HD // N_TP
    attended_groups = attended.reshape(SEQUENCE_LENGTH, N_TP, group_width).transpose(1, 0, 2)
    out_groups = out_weight.reshape(N_TP, group_width, D)

    def add_group(total, pair):
        return (total + rounded(jnp.dot(pair[0], pair[1], preferred_element_type=jnp.float32)), None)
    mixed = lax.scan(add_group, jnp.zeros((SEQUENCE_LENGTH, D), jnp.float32), (attended_groups, out_groups))[0]
    first_out = layer_norm(ALPHA * residual_in.astype(jnp.float32) + mixed, first_gain, first_shift).astype(jnp.bfloat16)
    hidden_width = FF // N_TP
    up_groups = up_weight.reshape(D, N_TP, hidden_width).transpose(1, 0, 2)
    down_groups = down_weight.reshape(D, N_TP, hidden_width).transpose(1, 0, 2)

    def add_hidden(total, pair):
        activated = jnp.square(jax.nn.relu(jnp.dot(first_out, pair[0], preferred_element_type=jnp.float32))).astype(jnp.bfloat16)
        partial_value = lax.dot_general(activated, pair[1], (((1,), (1,)), ((), ())), preferred_element_type=jnp.float32)
        return (total + rounded(partial_value), None)
    channel_mix = lax.scan(add_hidden, jnp.zeros((SEQUENCE_LENGTH, D), jnp.float32), (up_groups, down_groups))[0]
    second = layer_norm(ALPHA * first_out.astype(jnp.float32) + channel_mix, second_gain, second_shift)
    return second.astype(jnp.bfloat16)
```

```python
import functools
import math

import jax
import jax.numpy as jnp
from jax import lax
from jax.experimental import pallas as pl
from jax.experimental.pallas import tpu as pltpu
from jax.sharding import PartitionSpec as P

MESH = pl.DeviceIdType.MESH
ALPHA = 2.0**0.25
EPSILON = 1e-05
LOG2E = math.log2(math.e)
CLAMP = 120.0
F32 = jnp.float32
BF16 = jnp.bfloat16
NT = (((1,), (1,)), ((), ()))


def split_sp(n_sp):
    ny = 4 if n_sp == 32 else 2
    return n_sp // ny, ny


def iota(shape, dim):
    return lax.broadcasted_iota(jnp.int32, shape, dim)


class Mail:
    def __init__(self, send, recv):
        self.send, self.recv = send, recv

    def make(self, m, src, dst, target):
        return pltpu.make_async_remote_copy(
            src_ref=src,
            dst_ref=dst,
            send_sem=self.send.at[m],
            recv_sem=self.recv.at[m],
            device_id=target,
            device_id_type=MESH,
        )

    def start(self, m, src, dst, target):
        self.make(m, src, dst, target).start()

    def arrived(self, m, dst, target):
        self.make(m, dst, dst, target).wait_recv()

    def sent(self, m, src, target):
        self.make(m, src, src, target).wait_send()


class Gather:
    def __init__(self, mail, base, slot, nx):
        self.mail, self.base, self.slot, self.nx = mail, base, slot, nx
        me = lax.axis_index("tp")
        self.me, self.x, self.c = me, me // 2, me % 2
        self.sib = {"tp": self.x * 2 + 1 - self.c}

    @staticmethod
    def count(nx):
        return 2 * nx

    def at(self, r, core):
        return lax.rem(self.x + self.nx + r, self.nx) * 2 + core

    def start(self, src):
        for r in range(1, self.nx):
            self.mail.start(self.base + r, src, self.slot(self.me), {"tp": self.at(r, self.c)})
        self.mail.start(self.base, src, self.slot(self.me), self.sib)

    def forward(self):
        for r in range(1, self.nx):
            got = self.slot(self.at(-r, self.c))
            self.mail.arrived(self.base + r, got, self.sib)
            self.mail.start(self.base + self.nx + r, got, got, self.sib)

    def finish(self):
        other = 1 - self.c
        self.mail.arrived(self.base, self.slot(self.at(0, other)), self.sib)
        for r in range(1, self.nx):
            self.mail.arrived(self.base + self.nx + r, self.slot(self.at(-r, other)), self.sib)

    def drain(self):
        for r in range(self.nx):
            self.mail.sent(self.base + r, self.slot(self.me), self.sib)
        for r in range(1, self.nx):
            self.mail.sent(self.base + self.nx + r, self.slot(self.me), self.sib)


def attention_kernel(
    nz, ny, nx,
    q_ref, k_ref, v_ref, b_ref, ow_ref, res_ref, gain_ref, shift_ref,
    fo_ref,
    qbuf, kb, vb, bb, tri, pacc, tcol, tt, fac, part, partf, prec, stage,
    ow_full, res_full, att_full, pre,
    msend, mrecv, ksend, krecv, vsend, vrecv,
):
    sp = lax.axis_index("sp")
    z, y = sp // ny, lax.rem(sp, ny)
    me = lax.axis_index("tp")
    tb, hd = k_ref.shape
    half = tb // 2
    rows = 2 * ny * half
    mail = Mail(msend, mrecv)
    kmail, vmail = Mail(ksend, krecv), Mail(vsend, vrecv)

    def zdev(zz):
        return {"sp": zz * ny + y}

    def ydev(r):
        return {"sp": z * ny + lax.rem(y + ny + r, ny)}

    mirror = zdev(nz - 1 - z)

    barrier = pltpu.get_barrier_semaphore()
    for r in range(1, nz):
        pl.semaphore_signal(barrier, inc=1, device_id=zdev(lax.rem(z + r, nz)), device_id_type=MESH)
    for r in range(1, ny):
        pl.semaphore_signal(barrier, inc=1, device_id=ydev(r), device_id_type=MESH)
    for r in range(1, 2 * nx):
        pl.semaphore_signal(
            barrier, inc=1, device_id={"tp": lax.rem(me + r, 2 * nx)}, device_id_type=MESH
        )
    pl.semaphore_wait(barrier, nz - 1 + ny - 1 + 2 * nx - 1)

    m_q1, m_q2, m_q2f = 0, ny, 2 * ny
    m_b = 3 * ny
    m_t = m_b + nz
    m_p = m_t + ny
    m_ret = m_p + ny
    g0 = m_ret + 1
    gn = Gather.count(nx)
    g_ow = Gather(mail, g0, lambda j: ow_full.at[pl.ds(j * hd, hd), :], nx)
    dw = res_ref.shape[1]
    g_res = Gather(
        mail, g0 + gn, lambda j: res_full.at[:, pl.ds(pl.multiple_of(j * dw, dw), dw)], nx
    )
    g_att = [
        Gather(
            mail,
            g0 + (2 + h) * gn,
            functools.partial(
                lambda h, j: att_full.at[pl.ds(h * half, half), pl.ds(pl.multiple_of(j * hd, hd), hd)], h
            ),
            nx,
        )
        for h in range(2)
    ]

    early, late = q_ref.at[pl.ds(0, half), :], q_ref.at[pl.ds(half, half), :]
    mail.start(m_q2, late, qbuf.at[ny + y], mirror)
    for r in range(1, ny):
        mail.start(m_q1 + r, early, qbuf.at[y], ydev(r))
    for r in range(1, nz):
        mail.start(m_b + r, b_ref, bb.at[z], zdev(lax.rem(z + r, nz)))
    right, left = zdev(lax.rem(z + 1, nz)), zdev(lax.rem(z + nz - 1, nz))
    kmail.start(1, k_ref, kb.at[1], right)
    kmail.start(2, k_ref, kb.at[2], left)
    vmail.start(1, v_ref, vb.at[1], right)
    vmail.start(2, v_ref, vb.at[2], left)
    g_ow.start(ow_ref)
    g_res.start(res_ref)

    qbuf[y] = q_ref[:half, :]
    bb[z] = b_ref[...]
    kb[0] = k_ref[...]
    vb[0] = v_ref[...]
    ow_full[pl.ds(me * hd, hd), :] = ow_ref[...]
    res_full[:, pl.ds(pl.multiple_of(me * dw, dw), dw)] = res_ref[...]
    tri[...] = (iota((tb, tb), 0) > iota((tb, tb), 1)).astype(BF16)
    tcol[...] = jnp.zeros_like(tcol)
    fac[...] = jnp.zeros_like(fac)

    mail.arrived(m_q2, qbuf.at[ny + y], mirror)
    for r in range(1, ny):
        mail.start(m_q2f + r, qbuf.at[ny + y], qbuf.at[ny + y], ydev(r))
    for r in range(1, ny):
        mail.arrived(m_q1 + r, qbuf.at[lax.rem(y + ny - r, ny)], ydev(r))
    for r in range(1, ny):
        mail.arrived(m_q2f + r, qbuf.at[ny + lax.rem(y + ny - r, ny)], ydev(r))
    for r in range(1, nz):
        mail.arrived(m_b + r, bb.at[lax.rem(z + nz - r, nz)], left)

    scale = hd ** (-0.5) * LOG2E
    hk = tb // 2
    lane = iota((half, 128), 1)

    @pl.loop(0, nz)
    def _(i):
        odd = lax.rem(i, 2)
        step = (i + 1) // 2
        zb = lax.rem(jnp.where(odd == 1, z - step, z + step) + nz, nz)
        onward = zdev(lax.rem(jnp.where(odd == 1, z + 1, z - 1) + nz, nz))

        @pl.when(i > 0)
        def _():
            kmail.arrived(i, kb.at[i], onward)
            vmail.arrived(i, vb.at[i], onward)

        @pl.when(jnp.logical_and(i >= 1, i <= nz - 4))
        def _():
            kmail.start(i + 2, kb.at[i], kb.at[i + 2], onward)
            vmail.start(i + 2, vb.at[i], vb.at[i + 2], onward)

        @pl.when(i == nz - 3)
        def _():
            kmail.start(nz - 1, kb.at[i], kb.at[nz - 1], onward)

        @pl.when(i == nz - 2)
        def _():
            vmail.start(nz - 1, vb.at[i], vb.at[nz - 1], onward)

        def tile(t, h, masked):
            where = pl.ds(pl.multiple_of(t * half, half), half)
            scores = lax.dot_general(qbuf[t], kb[i], NT, preferred_element_type=F32)
            logits = scores * scale + bb[zb][0:1, :]
            soft = jnp.maximum(
                jnp.log(1.0 + jnp.exp2(jnp.minimum(logits, CLAMP))) * LOG2E, logits
            )
            brk = logits - soft
            if masked:
                strict = iota((half, tb), 1) < iota((half, tb), 0) + h * half
                soft = jnp.where(strict, soft, 0.0)
            soft16 = soft.astype(BF16)
            later0 = jnp.dot(soft16, tri[:, :hk], preferred_element_type=F32)
            later1 = jnp.dot(soft16[:, hk:], tri[hk:, hk:], preferred_element_type=F32)
            w0 = jnp.exp2(brk[:, :hk] - later0)
            w1 = jnp.exp2(brk[:, hk:] - later1)
            if masked:
                w0 = jnp.where(strict[:, :hk], w0, 0.0)
                w1 = jnp.where(strict[:, hk:], w1, 0.0)
            pacc[zb, where, :] = jnp.dot(
                w0.astype(BF16), vb[i, :hk, :], preferred_element_type=F32
            ) + jnp.dot(w1.astype(BF16), vb[i, hk:, :], preferred_element_type=F32)
            total = later0[:, 0:1] + soft[:, 0:1]
            tcol[where, :] = jnp.where(lane == zb, total, tcol[where, :])

        @pl.loop(0, 2 * ny)
        def _(t):
            h = t // ny
            qz = jnp.where(h == 0, z, nz - 1 - z)
            qblock = qz * ny + lax.rem(t, ny)
            kblock = zb * ny + y

            @pl.when(kblock < qblock)
            def _():
                tile(t, h, False)

            @pl.when(kblock == qblock)
            def _():
                tile(t, h, True)

            @pl.when(kblock > qblock)
            def _():
                where = pl.ds(pl.multiple_of(t * half, half), half)
                pacc[zb, where, :] = jnp.zeros((half, hd), F32)

    @pl.loop(0, rows // 128)
    def _(n):
        at = pl.ds(pl.multiple_of(n * 128, 128), 128)
        tt[y, :, at] = tcol[at, :].T[:8, :]

    for r in range(1, ny):
        mail.start(m_t + r, tt.at[y], tt.at[y], ydev(r))
    g_ow.forward()
    g_res.forward()
    for r in range(1, ny):
        mail.arrived(m_t + r, tt.at[lax.rem(y + ny - r, ny)], ydev(r))
    every = tt[0]
    after = jnp.zeros_like(every)
    for yy in range(ny):
        if yy:
            every = every + tt[yy]
        after = after + jnp.where(yy > y, tt[yy], 0.0)
    beyond = jnp.zeros_like(every[0:1, :])
    for zz in reversed(range(nz)):
        fac[zz : zz + 1, :] = jnp.exp2(-(beyond + after[zz : zz + 1, :]))
        beyond = beyond + every[zz : zz + 1, :]

    chunk = min(128, half)
    per = half // chunk

    @pl.loop(0, rows // 128)
    def _(n):
        at = pl.ds(pl.multiple_of(n * 128, 128), 128)
        cols = fac[:, at].T
        acc = cols[:, 0:1] * pacc[0, at, :]
        for zz in range(1, nz):
            acc = acc + cols[:, zz : zz + 1] * pacc[zz, at, :]
        partf[at, :] = acc
        part[at, :] = acc.astype(BF16)

    for r in range(1, ny):
        for h in range(2):
            to = lax.rem(y + r, ny)
            src = part.at[pl.ds(pl.multiple_of((h * ny + to) * half, half), half), :]
            mail.start(m_p + r if h == 0 else m_p2(m_p, r, g0, gn), src, prec.at[y, h], ydev(r))
    own = lambda h: partf[pl.ds(pl.multiple_of((h * ny + y) * half, half), half), :]

    def summed(h):
        acc = own(h)
        for r in range(1, ny):
            frm = lax.rem(y + ny - r, ny)
            mail.arrived(m_p + r if h == 0 else m_p2(m_p, r, g0, gn), prec.at[frm, h], ydev(r))
            acc = acc + prec[frm, h].astype(F32)
        return acc.astype(BF16)

    mycol = pl.ds(pl.multiple_of(me * hd, hd), hd)
    stage[...] = summed(1)
    mail.start(m_ret, stage, att_full.at[pl.ds(half, half), mycol], mirror)
    att_full[:half, mycol] = summed(0)
    g_att[0].start(att_full.at[pl.ds(0, half), mycol])
    mail.arrived(m_ret, att_full.at[pl.ds(half, half), mycol], mirror)
    g_att[1].start(att_full.at[pl.ds(half, half), mycol])
    g_ow.finish()
    g_res.finish()
    g_att[0].forward()
    g_att[1].forward()
    g_att[0].finish()
    g_att[1].finish()

    width = ow_full.shape[1]
    nc = min(256, width)

    @pl.loop(0, width // nc)
    def _(n):
        at = pl.ds(pl.multiple_of(n * nc, nc), nc)
        pre[:, at] = jnp.dot(att_full[...], ow_full[:, at], preferred_element_type=F32) + (
            ALPHA * res_full[:, at].astype(F32)
        )

    rc = 64

    @pl.loop(0, tb // rc)
    def _(n):
        at = pl.ds(pl.multiple_of(n * rc, rc), rc)
        row = pre[at, :]
        center = jnp.mean(row, axis=-1, keepdims=True)
        off = row - center
        spread = jnp.mean(off * off, axis=-1, keepdims=True)
        fo_ref[at, :] = (off * lax.rsqrt(spread + EPSILON) * gain_ref[...] + shift_ref[...]).astype(
            BF16
        )

    mail.sent(m_q2, late, mirror)
    for r in range(1, ny):
        mail.sent(m_q1 + r, early, mirror)
        mail.sent(m_q2f + r, early, mirror)
        mail.sent(m_t + r, tt.at[y], mirror)
        mail.sent(m_p + r, stage, mirror)
        mail.sent(m_p2(m_p, r, g0, gn), stage, mirror)
    for r in range(1, nz):
        mail.sent(m_b + r, b_ref, mirror)
    mail.sent(m_ret, stage, mirror)

    @pl.loop(1, nz)
    def _(i):
        kmail.sent(i, kb.at[0], mirror)
        vmail.sent(i, vb.at[0], mirror)

    for g in [g_ow, g_res] + g_att:
        g.drain()


def m_p2(m_p, r, g0, gn):
    return g0 + 4 * gn + r


def attention_layer(nz, ny, nx, q, k, v, bias, ow, res, gain, shift):
    tb, hd = q.shape
    half = tb // 2
    rows = 2 * ny * half
    width = ow.shape[1]
    ntp = 2 * nx
    gn = Gather.count(nx)
    messages = 3 * ny + nz + 2 * ny + 1 + 4 * gn + ny
    vm = pl.BlockSpec(memory_space=pltpu.VMEM)
    dma = pltpu.SemaphoreType.DMA
    return pl.pallas_call(
        functools.partial(attention_kernel, nz, ny, nx),
        out_shape=jax.ShapeDtypeStruct((tb, width), BF16),
        in_specs=[vm] * 8,
        out_specs=vm,
        scratch_shapes=[
            pltpu.VMEM((2 * ny, half, hd), BF16),
            pltpu.VMEM((nz, tb, hd), BF16),
            pltpu.VMEM((nz, tb, hd), BF16),
            pltpu.VMEM((nz, 8, tb), F32),
            pltpu.VMEM((tb, tb), BF16),
            pltpu.VMEM((nz, rows, hd), F32),
            pltpu.VMEM((rows, 128), F32),
            pltpu.VMEM((ny, 8, rows), F32),
            pltpu.VMEM((128, rows), F32),
            pltpu.VMEM((rows, hd), BF16),
            pltpu.VMEM((rows, hd), F32),
            pltpu.VMEM((ny, 2, half, hd), BF16),
            pltpu.VMEM((half, hd), BF16),
            pltpu.VMEM((ntp * hd, width), BF16),
            pltpu.VMEM((tb, width), BF16),
            pltpu.VMEM((tb, ntp * hd), BF16),
            pltpu.VMEM((tb, width), F32),
            dma((messages,)),
            dma((messages,)),
            dma((nz,)),
            dma((nz,)),
            dma((nz,)),
            dma((nz,)),
        ],
        compiler_params=pltpu.CompilerParams(
            collective_id=0, has_side_effects=True, vmem_limit_bytes=56 * 1024 * 1024
        ),
        cost_estimate=pl.CostEstimate(flops=20_000_000_000, bytes_accessed=8_000_000, transcendentals=0),
        name="attention_layer",
    )(q, k, v, bias, ow, res, gain, shift)


def up_kernel(x_ref, w_ref, o_ref):
    hidden = jnp.maximum(jnp.dot(x_ref[...], w_ref[...], preferred_element_type=F32), 0.0)
    o_ref[...] = (hidden * hidden).astype(BF16)


def up_project(x, w):
    tb, d = x.shape
    n = w.shape[1]
    nb = min(256, n)
    return pl.pallas_call(
        up_kernel,
        out_shape=jax.ShapeDtypeStruct((tb, n), BF16),
        grid=(n // nb,),
        in_specs=[
            pl.BlockSpec((tb, d), lambda i: (0, 0)),
            pl.BlockSpec((d, nb), lambda i: (0, i)),
        ],
        out_specs=pl.BlockSpec((tb, nb), lambda i: (0, i)),
        compiler_params=pltpu.CompilerParams(vmem_limit_bytes=24 * 1024 * 1024),
        cost_estimate=pl.CostEstimate(
            flops=2 * tb * d * n, bytes_accessed=2 * (tb * d + d * n + tb * n), transcendentals=0
        ),
        name="up_project",
    )(x, w)


def down_kernel(
    nx,
    act_ref, dw_ref, fo_ref, gain_ref, shift_ref,
    out_ref,
    sbuf, sib, xbuf, rbuf, mine, cols, stat,
    ssend, srecv, xsend, xrecv, tsend, trecv,
):
    me = lax.axis_index("tp")
    x, c = me // 2, lax.rem(me, 2)
    ntp = 2 * nx
    tb, dw = out_ref.shape
    smail, xmail, tmail = Mail(ssend, srecv), Mail(xsend, xrecv), Mail(tsend, trecv)
    sibling = {"tp": x * 2 + 1 - c}

    barrier = pltpu.get_barrier_semaphore()
    for r in range(1, ntp):
        pl.semaphore_signal(
            barrier, inc=1, device_id={"tp": lax.rem(me + r, ntp)}, device_id_type=MESH
        )
    pl.semaphore_wait(barrier, ntp - 1)

    @pl.loop(0, ntp)
    def _(i):
        first = i < nx
        n = lax.rem(i, nx)
        chip = lax.rem(x + 1 + n, nx)
        j = chip * 2 + jnp.where(first, 1 - c, c)
        piece = lax.dot_general(
            act_ref[...],
            dw_ref[pl.ds(pl.multiple_of(j * dw, dw), dw), :],
            NT,
            preferred_element_type=F32,
        )

        @pl.when(first)
        def _():
            sbuf[n] = piece.astype(BF16)
            smail.start(n, sbuf.at[n], sib.at[n], sibling)

        @pl.when(jnp.logical_not(first))
        def _():
            smail.arrived(n, sib.at[n], sibling)
            both = piece + sib[n].astype(F32)

            @pl.when(n < nx - 1)
            def _():
                xbuf[n] = both.astype(BF16)
                xmail.start(n, xbuf.at[n], rbuf.at[n], {"tp": j})

            @pl.when(n == nx - 1)
            def _():
                mine[...] = both

    at = pl.ds(pl.multiple_of(me * dw, dw), dw)
    total = mine[...] + ALPHA * fo_ref[:, at].astype(F32)
    for n in range(nx - 1):
        xmail.arrived(n, rbuf.at[n], sibling)
        total = total + rbuf[n].astype(F32)
    mine[...] = total
    row_sum = jnp.sum(total, axis=-1, keepdims=True)
    row_squares = jnp.sum(total * total, axis=-1, keepdims=True)
    lane = iota((tb, 128), 1)
    cols[...] = jnp.where(lane == 0, row_sum, jnp.where(lane == 1, row_squares, 0.0))
    for n in range(tb // 128):
        stat[me, :, n * 128 : (n + 1) * 128] = cols[n * 128 : (n + 1) * 128, :].T[:8, :]
    for r in range(1, ntp):
        tmail.start(r, stat.at[me], stat.at[me], {"tp": lax.rem(me + r, ntp)})
    for r in range(1, ntp):
        tmail.arrived(r, stat.at[lax.rem(me + ntp - r, ntp)], sibling)
    sums = stat[0]
    for j in range(1, ntp):
        sums = sums + stat[j]
    d = float(dw * ntp)
    padded = jnp.concatenate([sums, jnp.zeros((120, tb), F32)], axis=0)
    for n in range(tb // 128):
        rows = slice(n * 128, (n + 1) * 128)
        both = padded[:, rows].T
        center = both[:, 0:1] / d
        spread = both[:, 1:2] / d - center * center
        out_ref[rows, :] = (
            (mine[rows, :] - center) * lax.rsqrt(spread + EPSILON) * gain_ref[:, at] + shift_ref[:, at]
        ).astype(BF16)

    for n in range(nx):
        smail.sent(n, sbuf.at[n], sibling)
    for n in range(nx - 1):
        xmail.sent(n, xbuf.at[n], sibling)
    for r in range(1, ntp):
        tmail.sent(r, stat.at[me], sibling)


def down_project(nx, act, dw, fo, gain, shift):
    tb = act.shape[0]
    width = fo.shape[1]
    ntp = 2 * nx
    w = width // ntp
    vm = pl.BlockSpec(memory_space=pltpu.VMEM)
    dma = pltpu.SemaphoreType.DMA
    return pl.pallas_call(
        functools.partial(down_kernel, nx),
        out_shape=jax.ShapeDtypeStruct((tb, w), BF16),
        in_specs=[vm] * 5,
        out_specs=vm,
        scratch_shapes=[
            pltpu.VMEM((nx, tb, w), BF16),
            pltpu.VMEM((nx, tb, w), BF16),
            pltpu.VMEM((nx - 1, tb, w), BF16),
            pltpu.VMEM((nx - 1, tb, w), BF16),
            pltpu.VMEM((tb, w), F32),
            pltpu.VMEM((tb, 128), F32),
            pltpu.VMEM((ntp, 8, tb), F32),
            dma((nx,)),
            dma((nx,)),
            dma((nx,)),
            dma((nx,)),
            dma((ntp,)),
            dma((ntp,)),
        ],
        compiler_params=pltpu.CompilerParams(
            collective_id=1, has_side_effects=True, vmem_limit_bytes=32 * 1024 * 1024
        ),
        cost_estimate=pl.CostEstimate(flops=4_000_000_000, bytes_accessed=8_000_000, transcendentals=0),
        name="down_project",
    )(act, dw, fo, gain, shift)


def body(nz, ny, nx, queries, keys, values, breaks, residual_in, out_weight, first_gain,
         first_shift, up_weight, down_weight, second_gain, second_shift):
    up_full = lax.all_gather(up_weight, "sp", axis=0, tiled=True)
    down_full = lax.all_gather(down_weight, "sp", axis=0, tiled=True)
    bias = jnp.broadcast_to((breaks.astype(F32) * LOG2E).reshape(1, -1), (8, breaks.shape[0]))
    row = lambda a: a.reshape(1, -1)
    first_out = attention_layer(
        nz, ny, nx, queries, keys, values, bias, out_weight, residual_in,
        row(first_gain), row(first_shift),
    )
    activated = up_project(first_out, up_full)
    return down_project(
        nx, activated, down_full, first_out, row(second_gain), row(second_shift)
    )


def solution(mesh):
    nz, ny = split_sp(mesh.shape["sp"])
    nx = mesh.shape["tp"] // 2
    return jax.shard_map(
        functools.partial(body, nz, ny, nx),
        mesh=mesh,
        in_specs=(
            P("sp", "tp"),
            P("sp", "tp"),
            P("sp", "tp"),
            P("sp", "tp"),
            P("sp", "tp"),
            P("tp", None),
            P(),
            P(),
            P("sp", "tp"),
            P("sp", "tp"),
            P(),
            P(),
        ),
        out_specs=P("sp", "tp"),
        check_vma=False,
    )
```

```python
import functools
import math

import jax
import jax.numpy as jnp
from jax import lax
from jax.experimental import pallas as pl
from jax.experimental.pallas import tpu as pltpu
from jax.sharding import PartitionSpec as P

MESH = pl.DeviceIdType.MESH
ALPHA = 2.0**0.25
EPSILON = 1e-05
LOG2E = math.log2(math.e)
CLAMP = 120.0
F32 = jnp.float32
BF16 = jnp.bfloat16
NT = (((1,), (1,)), ((), ()))


def split_sp(n_sp):
    ny = 4 if n_sp >= 16 else 2
    return n_sp // ny, ny


def iota(shape, dim):
    return lax.broadcasted_iota(jnp.int32, shape, dim)


class Mail:
    def __init__(self, send, recv):
        self.send, self.recv = send, recv

    def make(self, m, src, dst, target, there=None):
        return pltpu.make_async_remote_copy(
            src_ref=src,
            dst_ref=dst,
            send_sem=self.send.at[m],
            recv_sem=self.recv.at[m if there is None else there],
            device_id=target,
            device_id_type=MESH,
        )

    def start(self, m, src, dst, target, there=None):
        self.make(m, src, dst, target, there).start()

    def arrived(self, m, dst, target):
        self.make(m, dst, dst, target).wait_recv()

    def sent(self, m, src, target):
        self.make(m, src, src, target).wait_send()


class Gather:
    def __init__(self, mail, base, slot, nx):
        self.mail, self.base, self.slot, self.nx = mail, base, slot, nx
        me = lax.axis_index("tp")
        self.me, self.x, self.c = me, me // 2, me % 2
        self.sib = {"tp": self.x * 2 + 1 - self.c}

    @staticmethod
    def count(nx):
        return 2 * nx

    def at(self, r, core):
        return lax.rem(self.x + self.nx + r, self.nx) * 2 + core

    def start(self, src):
        for r in range(1, self.nx):
            self.mail.start(self.base + r, src, self.slot(self.me), {"tp": self.at(r, self.c)})
        self.mail.start(self.base, src, self.slot(self.me), self.sib)

    def forward(self):
        for r in range(1, self.nx):
            got = self.slot(self.at(-r, self.c))
            self.mail.arrived(self.base + r, got, self.sib)
            self.mail.start(self.base + self.nx + r, got, got, self.sib)

    def finish(self):
        other = 1 - self.c
        self.mail.arrived(self.base, self.slot(self.at(0, other)), self.sib)
        for r in range(1, self.nx):
            self.mail.arrived(self.base + self.nx + r, self.slot(self.at(-r, other)), self.sib)

    def drain(self):
        for r in range(self.nx):
            self.mail.sent(self.base + r, self.slot(self.me), self.sib)
        for r in range(1, self.nx):
            self.mail.sent(self.base + self.nx + r, self.slot(self.me), self.sib)


def layer_kernel(
    nz, ny, nx,
    q_ref, k_ref, v_ref, b_ref, ow_ref, res_ref, gain_ref, shift_ref,
    uw_ref, dw_ref, gain2_ref, shift2_ref,
    out_ref,
    qbuf, kb, vb, bb, tri, pacc, tcol, tt, fac, part, partf, prec, stage,
    ow_full, res_full, att_full, pre, fo_ref,
    up_full, down_full, act, hold, sbuf, sib, xbuf, rbuf, mine, cols, stat,
    msend, mrecv, ksend, krecv, vsend, vrecv,
    usend, urecv, ysend, yrecv, dsend, drecv,
    ssend, srecv, xsend, xrecv, tsend, trecv,
):
    sp = lax.axis_index("sp")
    z, y = sp // ny, lax.rem(sp, ny)
    me = lax.axis_index("tp")
    tb, hd = k_ref.shape
    half = tb // 2
    rows = 2 * ny * half
    mail = Mail(msend, mrecv)
    kmail, vmail = Mail(ksend, krecv), Mail(vsend, vrecv)
    umail, ymail, dmail = Mail(usend, urecv), Mail(ysend, yrecv), Mail(dsend, drecv)
    wr = uw_ref.shape[0]

    def zdev(zz):
        return {"sp": zz * ny + y}

    def ydev(r):
        return {"sp": z * ny + lax.rem(y + ny + r, ny)}

    mirror = zdev(nz - 1 - z)

    def zof(i):
        odd, step = lax.rem(i, 2), (i + 1) // 2
        return lax.rem(jnp.where(odd == 1, z - step, z + step) + nz, nz)

    def up_slab(zz, r, part=None):
        at = (zz * ny + lax.rem(y + ny + r, ny)) * wr
        n = wr if part is None else wr // 2
        return up_full.at[pl.ds(pl.multiple_of(at + (part or 0) * n, n), n), :]

    dh = ny * wr // 2

    def down_half(zz, h):
        return down_full.at[pl.ds(pl.multiple_of((zz * 2 + h) * dh, dh), dh), :]

    def down_slab(r):
        at = (z * ny + lax.rem(y + ny + r, ny)) * wr
        return down_full.at[pl.ds(pl.multiple_of(at, wr), wr), :]

    barrier = pltpu.get_barrier_semaphore()
    for r in range(1, nz):
        pl.semaphore_signal(barrier, inc=1, device_id=zdev(lax.rem(z + r, nz)), device_id_type=MESH)
    for r in range(1, ny):
        pl.semaphore_signal(barrier, inc=1, device_id=ydev(r), device_id_type=MESH)
    for r in range(1, 2 * nx):
        pl.semaphore_signal(
            barrier, inc=1, device_id={"tp": lax.rem(me + r, 2 * nx)}, device_id_type=MESH
        )
    pl.semaphore_wait(barrier, nz - 1 + ny - 1 + 2 * nx - 1)

    m_q1, m_q2, m_q2f = 0, ny, 2 * ny
    m_b = 3 * ny
    m_t = m_b + nz
    m_p = m_t + ny
    m_ret = m_p + ny
    m_d = m_ret + 1
    g0 = m_d + ny
    gn = Gather.count(nx)
    g_ow = Gather(mail, g0, lambda j: ow_full.at[pl.ds(j * hd, hd), :], nx)
    dw = res_ref.shape[1]
    g_res = Gather(
        mail, g0 + gn, lambda j: res_full.at[:, pl.ds(pl.multiple_of(j * dw, dw), dw)], nx
    )
    g_att = [
        Gather(
            mail,
            g0 + (2 + h) * gn,
            functools.partial(
                lambda h, j: att_full.at[pl.ds(h * half, half), pl.ds(pl.multiple_of(j * hd, hd), hd)], h
            ),
            nx,
        )
        for h in range(2)
    ]

    early, late = q_ref.at[pl.ds(0, half), :], q_ref.at[pl.ds(half, half), :]
    mail.start(m_q2, late, qbuf.at[ny + y], mirror)
    for r in range(1, ny):
        mail.start(m_q1 + r, early, qbuf.at[y], ydev(r))
    for r in range(1, nz):
        mail.start(m_b + r, b_ref, bb.at[z], zdev(lax.rem(z + r, nz)))
    right, left = zdev(lax.rem(z + 1, nz)), zdev(lax.rem(z + nz - 1, nz))
    kmail.start(1, k_ref, kb.at[1], right)
    kmail.start(2, k_ref, kb.at[2], left)
    vmail.start(1, v_ref, vb.at[1], right)
    vmail.start(2, v_ref, vb.at[2], left)
    umail.start(1, uw_ref, up_slab(z, 0), right)
    umail.start(2, uw_ref, up_slab(z, 0), left)
    for r in range(1, ny):
        mail.start(m_d + r, dw_ref, down_slab(0), ydev(r))

    def pass_up(i, src):
        slab = up_slab(zof(i), 0)
        ymail.start(4 * i, slab if src is None else src, slab, ydev(1))
        if ny > 2:
            ymail.start(4 * i + 1, slab if src is None else src, slab, ydev(-1))

    def relay_up(i):
        if ny > 2:
            zz = zof(i)
            ymail.arrived(4 * i, up_slab(zz, -1), ydev(-1))
            ymail.start(4 * i + 2, up_slab(zz, -1, 0), up_slab(zz, -1, 0), ydev(1))
            ymail.arrived(4 * i + 1, up_slab(zz, 1), ydev(1))
            ymail.start(4 * i + 3, up_slab(zz, 1, 1), up_slab(zz, 1, 1), ydev(-1))

    def take_up(i):
        zz = zof(i)
        if ny > 2:
            ymail.arrived(4 * i + 2, up_slab(zz, -2, 0), ydev(-1))
            ymail.arrived(4 * i + 3, up_slab(zz, 2, 1), ydev(1))
        else:
            ymail.arrived(4 * i, up_slab(zz, -1), ydev(-1))

    pass_up(0, uw_ref)
    g_ow.start(ow_ref)
    g_res.start(res_ref)
    up_slab(z, 0)[...] = uw_ref[...]
    down_slab(0)[...] = dw_ref[...]

    qbuf[y] = q_ref[:half, :]
    bb[z] = b_ref[...]
    kb[0] = k_ref[...]
    vb[0] = v_ref[...]
    ow_full[pl.ds(me * hd, hd), :] = ow_ref[...]
    res_full[:, pl.ds(pl.multiple_of(me * dw, dw), dw)] = res_ref[...]
    tri[...] = (iota((tb, tb), 0) > iota((tb, tb), 1)).astype(BF16)
    tcol[...] = jnp.zeros_like(tcol)
    fac[...] = jnp.zeros_like(fac)

    mail.arrived(m_q2, qbuf.at[ny + y], mirror)
    for r in range(1, ny):
        mail.start(m_q2f + r, qbuf.at[ny + y], qbuf.at[ny + y], ydev(r))
    for r in range(1, ny):
        mail.arrived(m_q1 + r, qbuf.at[lax.rem(y + ny - r, ny)], ydev(r))
    for r in range(1, ny):
        mail.arrived(m_q2f + r, qbuf.at[ny + lax.rem(y + ny - r, ny)], ydev(r))
    for r in range(1, nz):
        mail.arrived(m_b + r, bb.at[lax.rem(z + nz - r, nz)], left)

    scale = hd ** (-0.5) * LOG2E
    hk = tb // 2
    lane = iota((half, 128), 1)

    @pl.loop(0, nz)
    def _(i):
        odd = lax.rem(i, 2)
        zb = zof(i)
        onward = zdev(lax.rem(jnp.where(odd == 1, z + 1, z - 1) + nz, nz))

        @pl.when(i > 0)
        def _():
            kmail.arrived(i, kb.at[i], onward)
            vmail.arrived(i, vb.at[i], onward)

        @pl.when(jnp.logical_and(i >= 1, i <= nz - 4))
        def _():
            kmail.start(i + 2, kb.at[i], kb.at[i + 2], onward)
            vmail.start(i + 2, vb.at[i], vb.at[i + 2], onward)

        @pl.when(i == nz - 3)
        def _():
            kmail.start(nz - 1, kb.at[i], kb.at[nz - 1], onward)

        @pl.when(i == nz - 2)
        def _():
            vmail.start(nz - 1, vb.at[i], vb.at[nz - 1], onward)

        def tile(t, h, masked):
            where = pl.ds(pl.multiple_of(t * half, half), half)
            scores = lax.dot_general(qbuf[t], kb[i], NT, preferred_element_type=F32)
            logits = scores * scale + bb[zb][0:1, :]
            soft = jnp.maximum(
                jnp.log(1.0 + jnp.exp2(jnp.minimum(logits, CLAMP))) * LOG2E, logits
            )
            brk = logits - soft
            if masked:
                strict = iota((half, tb), 1) < iota((half, tb), 0) + h * half
                soft = jnp.where(strict, soft, 0.0)
            soft16 = soft.astype(BF16)
            later0 = jnp.dot(soft16, tri[:, :hk], preferred_element_type=F32)
            later1 = jnp.dot(soft16[:, hk:], tri[hk:, hk:], preferred_element_type=F32)
            w0 = jnp.exp2(brk[:, :hk] - later0)
            w1 = jnp.exp2(brk[:, hk:] - later1)
            if masked:
                w0 = jnp.where(strict[:, :hk], w0, 0.0)
                w1 = jnp.where(strict[:, hk:], w1, 0.0)
            pacc[zb, where, :] = jnp.dot(
                w0.astype(BF16), vb[i, :hk, :], preferred_element_type=F32
            ) + jnp.dot(w1.astype(BF16), vb[i, hk:, :], preferred_element_type=F32)
            total = later0[:, 0:1] + soft[:, 0:1]
            tcol[where, :] = jnp.where(lane == zb, total, tcol[where, :])

        @pl.loop(0, 2 * ny)
        def _(t):
            h = t // ny
            qz = jnp.where(h == 0, z, nz - 1 - z)
            qblock = qz * ny + lax.rem(t, ny)
            kblock = zb * ny + y

            @pl.when(kblock < qblock)
            def _():
                tile(t, h, False)

            @pl.when(kblock == qblock)
            def _():
                tile(t, h, True)

            @pl.when(kblock > qblock)
            def _():
                where = pl.ds(pl.multiple_of(t * half, half), half)
                pacc[zb, where, :] = jnp.zeros((half, hd), F32)

        @pl.when(jnp.logical_and(i > 0, i < nz - 1))
        def _():
            umail.arrived(i, up_slab(zb, 0), onward)

        @pl.when(jnp.logical_and(i >= 1, i <= nz - 4))
        def _():
            umail.start(i + 2, up_slab(zb, 0), up_slab(zb, 0), onward)

        @pl.when(i == nz - 3)
        def _():
            umail.start(nz - 1, up_slab(zb, 0, 0), up_slab(zb, 0, 0), onward)

        @pl.when(i == nz - 2)
        def _():
            umail.start(nz, up_slab(zb, 0, 1), up_slab(zb, 0, 1), onward)
            for r in range(1, ny):
                mail.arrived(m_d + r, down_slab(-r), ydev(r))
            for h in range(2):
                for j, to in ((1, right), (2, left)):
                    dmail.start(2 * j + h, down_half(z, h), down_half(z, h), to)

        @pl.when(jnp.logical_and(i > 0, i < nz - 1))
        def _():
            pass_up(i, None)

        @pl.when(i >= 2)
        def _():
            relay_up(i - 2)

    def down_step(step):
        for h in range(2):
            for i, to in ((2 * step - 1, right), (2 * step, left)):
                zz = zof(i)
                dmail.arrived(2 * i + h, down_half(zz, h), to)
                if i + 2 < nz - 1:
                    dmail.start(2 * (i + 2) + h, down_half(zz, h), down_half(zz, h), to)
                elif (i + h) % 2 == 1:
                    dmail.start(2 * (nz - 1) + h, down_half(zz, h), down_half(zz, h), to)

    @pl.loop(0, rows // 128)
    def _(n):
        at = pl.ds(pl.multiple_of(n * 128, 128), 128)
        tt[y, :, at] = tcol[at, :].T[:8, :]

    for r in range(1, ny):
        mail.start(m_t + r, tt.at[y], tt.at[y], ydev(r))
    last = zof(nz - 1)
    umail.arrived(nz - 1, up_slab(last, 0, 0), left)
    umail.arrived(nz, up_slab(last, 0, 1), right)
    pass_up(nz - 1, None)
    g_ow.forward()
    g_res.forward()
    for r in range(1, ny):
        mail.arrived(m_t + r, tt.at[lax.rem(y + ny - r, ny)], ydev(r))
    every = tt[0]
    after = jnp.zeros_like(every)
    for yy in range(ny):
        if yy:
            every = every + tt[yy]
        after = after + jnp.where(yy > y, tt[yy], 0.0)
    beyond = jnp.zeros_like(every[0:1, :])
    for zz in reversed(range(nz)):
        fac[zz : zz + 1, :] = jnp.exp2(-(beyond + after[zz : zz + 1, :]))
        beyond = beyond + every[zz : zz + 1, :]

    chunk = min(128, half)
    per = half // chunk

    @pl.loop(0, rows // 128)
    def _(n):
        at = pl.ds(pl.multiple_of(n * 128, 128), 128)
        cols = fac[:, at].T
        acc = cols[:, 0:1] * pacc[0, at, :]
        for zz in range(1, nz):
            acc = acc + cols[:, zz : zz + 1] * pacc[zz, at, :]
        partf[at, :] = acc
        part[at, :] = acc.astype(BF16)

    for r in range(1, ny):
        for h in range(2):
            to = lax.rem(y + r, ny)
            src = part.at[pl.ds(pl.multiple_of((h * ny + to) * half, half), half), :]
            mail.start(m_p + r if h == 0 else m_p2(m_p, r, g0, gn), src, prec.at[y, h], ydev(r))
    relay_up(nz - 2)
    own = lambda h: partf[pl.ds(pl.multiple_of((h * ny + y) * half, half), half), :]

    def summed(h):
        acc = own(h)
        for r in range(1, ny):
            frm = lax.rem(y + ny - r, ny)
            mail.arrived(m_p + r if h == 0 else m_p2(m_p, r, g0, gn), prec.at[frm, h], ydev(r))
            acc = acc + prec[frm, h].astype(F32)
        return acc.astype(BF16)

    mycol = pl.ds(pl.multiple_of(me * hd, hd), hd)
    stage[...] = summed(1)
    mail.start(m_ret, stage, att_full.at[pl.ds(half, half), mycol], mirror)
    relay_up(nz - 1)
    att_full[:half, mycol] = summed(0)
    g_att[0].start(att_full.at[pl.ds(0, half), mycol])
    if nz > 4:
        down_step(1)
    mail.arrived(m_ret, att_full.at[pl.ds(half, half), mycol], mirror)
    g_att[1].start(att_full.at[pl.ds(half, half), mycol])
    g_ow.finish()
    g_res.finish()
    g_att[0].forward()
    g_att[1].forward()
    g_att[0].finish()
    g_att[1].finish()

    width = ow_full.shape[1]
    nc = min(256, width)

    @pl.loop(0, width // nc)
    def _(n):
        at = pl.ds(pl.multiple_of(n * nc, nc), nc)
        pre[:, at] = jnp.dot(att_full[...], ow_full[:, at], preferred_element_type=F32) + (
            ALPHA * res_full[:, at].astype(F32)
        )

    if nz > 6:
        down_step(2)
    rc = 64

    @pl.loop(0, tb // rc)
    def _(n):
        at = pl.ds(pl.multiple_of(n * rc, rc), rc)
        row = pre[at, :]
        center = jnp.mean(row, axis=-1, keepdims=True)
        off = row - center
        spread = jnp.mean(off * off, axis=-1, keepdims=True)
        fo_ref[at, :] = (off * lax.rsqrt(spread + EPSILON) * gain_ref[...] + shift_ref[...]).astype(
            BF16
        )

    for i in range(nz):
        take_up(i)
    hidden = up_full.shape[1]
    hc = min(256, hidden)

    @pl.loop(0, hidden // hc)
    def _(n):
        at = pl.ds(pl.multiple_of(n * hc, hc), hc)
        h = jnp.maximum(jnp.dot(fo_ref[...], up_full[:, at], preferred_element_type=F32), 0.0)
        act[:, at] = (h * h).astype(BF16)

    ntp = 2 * nx
    x, c = me // 2, lax.rem(me, 2)
    smail, xmail, tmail = Mail(ssend, srecv), Mail(xsend, xrecv), Mail(tsend, trecv)
    sibling = {"tp": x * 2 + 1 - c}
    fw = out_ref.shape[1]

    def mix(i):
        j = zof(i)
        chip = j // 2
        piece = lax.dot_general(
            act[...],
            down_full[pl.ds(pl.multiple_of(j * fw, fw), fw), :],
            NT,
            preferred_element_type=F32,
        )

        @pl.when(lax.rem(j, 2) != c)
        def _():
            sbuf[chip] = piece.astype(BF16)
            smail.start(chip, sbuf.at[chip], sib.at[chip], sibling)

        @pl.when(lax.rem(j, 2) == c)
        def _():
            hold[...] = piece

    def settle(i):
        j = zof(i)
        chip = j // 2

        @pl.when(lax.rem(j, 2) == c)
        def _():
            smail.arrived(chip, sib.at[chip], sibling)
            both = hold[...] + sib[chip].astype(F32)

            @pl.when(chip != x)
            def _():
                xbuf[chip] = both.astype(BF16)
                xmail.start(chip, xbuf.at[chip], rbuf.at[x], {"tp": j}, there=x)

            @pl.when(chip == x)
            def _():
                mine[...] = both

    final = nz // 2 - 1

    @pl.loop(0, nz)
    def _(i):
        @pl.when(i == nz - 3)
        def _():
            down_step(final)

        @pl.when(i == nz - 1)
        def _():
            zz = zof(nz - 1)
            dmail.arrived(2 * (nz - 1), down_half(zz, 0), left)
            dmail.arrived(2 * (nz - 1) + 1, down_half(zz, 1), right)

        mix(i)
        settle(i)

    at = pl.ds(pl.multiple_of(me * fw, fw), fw)
    mine[...] = mine[...] + ALPHA * fo_ref[:, at].astype(F32)
    for r in range(1, nx):
        n = lax.rem(x + r, nx)
        xmail.arrived(n, rbuf.at[n], sibling)
        mine[...] = mine[...] + rbuf[n].astype(F32)
    total = mine[...]
    row_sum = jnp.sum(total, axis=-1, keepdims=True)
    row_squares = jnp.sum(total * total, axis=-1, keepdims=True)
    lane = iota((tb, 128), 1)
    cols[...] = jnp.where(lane == 0, row_sum, jnp.where(lane == 1, row_squares, 0.0))
    for n in range(tb // 128):
        stat[me, :, n * 128 : (n + 1) * 128] = cols[n * 128 : (n + 1) * 128, :].T[:8, :]
    for r in range(1, ntp):
        tmail.start(r, stat.at[me], stat.at[me], {"tp": lax.rem(me + r, ntp)})
    for r in range(1, ntp):
        tmail.arrived(r, stat.at[lax.rem(me + ntp - r, ntp)], sibling)
    sums = stat[0]
    for j in range(1, ntp):
        sums = sums + stat[j]
    d = float(fw * ntp)
    padded = jnp.concatenate([sums, jnp.zeros((120, tb), F32)], axis=0)
    for n in range(tb // 128):
        rows_n = slice(n * 128, (n + 1) * 128)
        both = padded[:, rows_n].T
        center = both[:, 0:1] / d
        spread = both[:, 1:2] / d - center * center
        out_ref[rows_n, :] = (
            (mine[rows_n, :] - center) * lax.rsqrt(spread + EPSILON) * gain2_ref[:, at]
            + shift2_ref[:, at]
        ).astype(BF16)

    mail.sent(m_q2, late, mirror)
    for r in range(1, ny):
        mail.sent(m_q1 + r, early, mirror)
        mail.sent(m_q2f + r, early, mirror)
        mail.sent(m_t + r, tt.at[y], mirror)
        mail.sent(m_p + r, stage, mirror)
        mail.sent(m_p2(m_p, r, g0, gn), stage, mirror)
    for r in range(1, nz):
        mail.sent(m_b + r, b_ref, mirror)
    mail.sent(m_ret, stage, mirror)
    for r in range(1, ny):
        mail.sent(m_d + r, dw_ref, mirror)
    for i in range(1, nz + 1):
        umail.sent(i, up_slab(0, 0) if i < nz - 1 else up_slab(0, 0, 0), mirror)
    for i in range(nz):
        ymail.sent(4 * i, up_slab(0, 0), mirror)
        if ny > 2:
            ymail.sent(4 * i + 1, up_slab(0, 0), mirror)
            ymail.sent(4 * i + 2, up_slab(0, 0, 0), mirror)
            ymail.sent(4 * i + 3, up_slab(0, 0, 0), mirror)
    for i in range(1, nz):
        for h in range(2):
            dmail.sent(2 * i + h, down_half(0, 0), mirror)
    for n in range(nx):
        smail.sent(n, sbuf.at[0], sibling)
    for r in range(1, nx):
        xmail.sent(lax.rem(x + r, nx), rbuf.at[0], sibling)
    for r in range(1, ntp):
        tmail.sent(r, stat.at[me], sibling)

    @pl.loop(1, nz)
    def _(i):
        kmail.sent(i, kb.at[0], mirror)
        vmail.sent(i, vb.at[0], mirror)

    for g in [g_ow, g_res] + g_att:
        g.drain()


def m_p2(m_p, r, g0, gn):
    return g0 + 4 * gn + r


def layer(nz, ny, nx, q, k, v, bias, ow, res, gain, shift, uw, dw, gain2, shift2):
    tb, hd = q.shape
    half = tb // 2
    rows = 2 * ny * half
    width = ow.shape[1]
    ntp = 2 * nx
    fw = width // ntp
    hidden = uw.shape[1]
    messages = 3 * ny + nz + 2 * ny + 1 + ny + 4 * Gather.count(nx) + ny
    vm = pl.BlockSpec(memory_space=pltpu.VMEM)
    dma = pltpu.SemaphoreType.DMA
    pairs = [messages, nz, nz, nz + 1, 4 * nz, 2 * nz, nx, nx, ntp]
    return pl.pallas_call(
        functools.partial(layer_kernel, nz, ny, nx),
        out_shape=jax.ShapeDtypeStruct((tb, fw), BF16),
        in_specs=[vm] * 12,
        out_specs=vm,
        scratch_shapes=[
            pltpu.VMEM((2 * ny, half, hd), BF16),
            pltpu.VMEM((nz, tb, hd), BF16),
            pltpu.VMEM((nz, tb, hd), BF16),
            pltpu.VMEM((nz, 8, tb), F32),
            pltpu.VMEM((tb, tb), BF16),
            pltpu.VMEM((nz, rows, hd), F32),
            pltpu.VMEM((rows, 128), F32),
            pltpu.VMEM((ny, 8, rows), F32),
            pltpu.VMEM((128, rows), F32),
            pltpu.VMEM((rows, hd), BF16),
            pltpu.VMEM((rows, hd), F32),
            pltpu.VMEM((ny, 2, half, hd), BF16),
            pltpu.VMEM((half, hd), BF16),
            pltpu.VMEM((ntp * hd, width), BF16),
            pltpu.VMEM((tb, width), BF16),
            pltpu.VMEM((tb, ntp * hd), BF16),
            pltpu.VMEM((tb, width), F32),
            pltpu.VMEM((tb, width), BF16),
            pltpu.VMEM((width, hidden), BF16),
            pltpu.VMEM((width, hidden), BF16),
            pltpu.VMEM((tb, hidden), BF16),
            pltpu.VMEM((tb, fw), F32),
            pltpu.VMEM((nx, tb, fw), BF16),
            pltpu.VMEM((nx, tb, fw), BF16),
            pltpu.VMEM((nx, tb, fw), BF16),
            pltpu.VMEM((nx, tb, fw), BF16),
            pltpu.VMEM((tb, fw), F32),
            pltpu.VMEM((tb, 128), F32),
            pltpu.VMEM((ntp, 8, tb), F32),
        ]
        + [dma((n,)) for n in pairs for _ in range(2)],
        compiler_params=pltpu.CompilerParams(
            collective_id=0, has_side_effects=True, vmem_limit_bytes=60 * 1024 * 1024
        ),
        name="layer",
    )(q, k, v, bias, ow, res, gain, shift, uw, dw, gain2, shift2)


def body(nz, ny, nx, queries, keys, values, breaks, residual_in, out_weight, first_gain,
         first_shift, up_weight, down_weight, second_gain, second_shift):
    bias = jnp.broadcast_to((breaks.astype(F32) * LOG2E).reshape(1, -1), (8, breaks.shape[0]))
    row = lambda a: a.reshape(1, -1)
    return layer(
        nz, ny, nx, queries, keys, values, bias, out_weight, residual_in,
        row(first_gain), row(first_shift), up_weight, down_weight, row(second_gain), row(second_shift),
    )


def solution(mesh):
    nz, ny = split_sp(mesh.shape["sp"])
    nx = mesh.shape["tp"] // 2
    return jax.shard_map(
        functools.partial(body, nz, ny, nx),
        mesh=mesh,
        in_specs=(
            P("sp", "tp"),
            P("sp", "tp"),
            P("sp", "tp"),
            P("sp", "tp"),
            P("sp", "tp"),
            P("tp", None),
            P(),
            P(),
            P("sp", "tp"),
            P("sp", "tp"),
            P(),
            P(),
        ),
        out_specs=P("sp", "tp"),
        check_vma=False,
    )
```

```python
import functools
import math

import jax
import jax.numpy as jnp
from jax import lax
from jax.experimental import pallas as pl
from jax.experimental.pallas import tpu as pltpu
from jax.sharding import PartitionSpec as P

MESH = pl.DeviceIdType.MESH
ALPHA = 2.0**0.25
EPSILON = 1e-05
LOG2E = math.log2(math.e)
CLAMP = 120.0
F32 = jnp.float32
BF16 = jnp.bfloat16
NT = (((1,), (1,)), ((), ()))


def split_sp(n_sp):
    ny = 4 if n_sp >= 16 else 2
    return n_sp // ny, ny


def iota(shape, dim):
    return lax.broadcasted_iota(jnp.int32, shape, dim)


class Mail:
    def __init__(self, send, recv):
        self.send, self.recv = send, recv

    def make(self, m, src, dst, target, there=None):
        return pltpu.make_async_remote_copy(
            src_ref=src,
            dst_ref=dst,
            send_sem=self.send.at[m],
            recv_sem=self.recv.at[m if there is None else there],
            device_id=target,
            device_id_type=MESH,
        )

    def start(self, m, src, dst, target, there=None):
        self.make(m, src, dst, target, there).start()

    def arrived(self, m, dst, target):
        self.make(m, dst, dst, target).wait_recv()

    def sent(self, m, src, target):
        self.make(m, src, src, target).wait_send()


class Gather:
    def __init__(self, mail, base, slot, nx):
        self.mail, self.base, self.slot, self.nx = mail, base, slot, nx
        me = lax.axis_index("tp")
        self.me, self.x, self.c = me, me // 2, me % 2
        self.sib = {"tp": self.x * 2 + 1 - self.c}

    @staticmethod
    def count(nx):
        return 2 * nx

    def at(self, r, core):
        return lax.rem(self.x + self.nx + r, self.nx) * 2 + core

    def start(self, src):
        for r in range(1, self.nx):
            self.mail.start(self.base + r, src, self.slot(self.me), {"tp": self.at(r, self.c)})
        self.mail.start(self.base, src, self.slot(self.me), self.sib)

    def forward(self):
        for r in range(1, self.nx):
            got = self.slot(self.at(-r, self.c))
            self.mail.arrived(self.base + r, got, self.sib)
            self.mail.start(self.base + self.nx + r, got, got, self.sib)

    def finish(self):
        other = 1 - self.c
        self.mail.arrived(self.base, self.slot(self.at(0, other)), self.sib)
        for r in range(1, self.nx):
            self.mail.arrived(self.base + self.nx + r, self.slot(self.at(-r, other)), self.sib)

    def drain(self):
        for r in range(self.nx):
            self.mail.sent(self.base + r, self.slot(self.me), self.sib)
        for r in range(1, self.nx):
            self.mail.sent(self.base + self.nx + r, self.slot(self.me), self.sib)


def layer_kernel(
    nz, ny, nx,
    q_ref, k_ref, v_ref, b_ref, ow_ref, res_ref, gain_ref, shift_ref,
    uw_ref, dw_ref, gain2_ref, shift2_ref,
    out_ref,
    qbuf, kb, vb, bb, tri, pacc, tt, fac, part, partf, prec,
    ow_full, res_full, att_full, pre, fo_ref,
    up_full, down_full, act, hold, sbuf, sib, xbuf, rbuf, mine, cols, stat,
    msend, mrecv, ksend, krecv, vsend, vrecv,
    usend, urecv, ysend, yrecv, dsend, drecv,
    ssend, srecv, xsend, xrecv, tsend, trecv,
):
    sp = lax.axis_index("sp")
    z, y = sp // ny, lax.rem(sp, ny)
    me = lax.axis_index("tp")
    tb, hd = k_ref.shape
    half = tb // 2
    rows = ny * tb
    mail = Mail(msend, mrecv)
    kmail, vmail = Mail(ksend, krecv), Mail(vsend, vrecv)
    umail, ymail, dmail = Mail(usend, urecv), Mail(ysend, yrecv), Mail(dsend, drecv)
    wr = uw_ref.shape[0]

    def zdev(zz):
        return {"sp": zz * ny + y}

    def ydev(r):
        return {"sp": z * ny + lax.rem(y + ny + r, ny)}

    def zof(i):
        odd, step = lax.rem(i, 2), (i + 1) // 2
        return lax.rem(jnp.where(odd == 1, z - step, z + step) + nz, nz)

    def up_slab(zz, r, part=None):
        at = (zz * ny + lax.rem(y + ny + r, ny)) * wr
        n = wr if part is None else wr // 2
        return up_full.at[pl.ds(pl.multiple_of(at + (part or 0) * n, n), n), :]

    dh = ny * wr // 2

    def down_half(zz, h):
        return down_full.at[pl.ds(pl.multiple_of((zz * 2 + h) * dh, dh), dh), :]

    def down_slab(r):
        at = (z * ny + lax.rem(y + ny + r, ny)) * wr
        return down_full.at[pl.ds(pl.multiple_of(at, wr), wr), :]

    barrier = pltpu.get_barrier_semaphore()
    for r in range(1, nz):
        pl.semaphore_signal(barrier, inc=1, device_id=zdev(lax.rem(z + r, nz)), device_id_type=MESH)
    for r in range(1, ny):
        pl.semaphore_signal(barrier, inc=1, device_id=ydev(r), device_id_type=MESH)
    for r in range(1, 2 * nx):
        pl.semaphore_signal(
            barrier, inc=1, device_id={"tp": lax.rem(me + r, 2 * nx)}, device_id_type=MESH
        )
    pl.semaphore_wait(barrier, nz - 1 + ny - 1 + 2 * nx - 1)

    m_q = 0
    m_b = ny
    m_t = m_b + nz
    m_p = m_t + ny
    m_d = m_p + ny
    g0 = m_d + ny
    gn = Gather.count(nx)
    g_ow = Gather(mail, g0, lambda j: ow_full.at[pl.ds(j * hd, hd), :], nx)
    dw = res_ref.shape[1]
    g_res = Gather(
        mail, g0 + gn, lambda j: res_full.at[:, pl.ds(pl.multiple_of(j * dw, dw), dw)], nx
    )
    g_att = [
        Gather(
            mail,
            g0 + (2 + h) * gn,
            functools.partial(
                lambda h, j: att_full.at[pl.ds(h * half, half), pl.ds(pl.multiple_of(j * hd, hd), hd)], h
            ),
            nx,
        )
        for h in range(2)
    ]

    right, left = zdev(lax.rem(z + 1, nz)), zdev(lax.rem(z + nz - 1, nz))
    kmail.start(1, k_ref, kb.at[1], right)
    kmail.start(2, k_ref, kb.at[2], left)
    for r in range(1, ny):
        mail.start(m_q + r, q_ref, qbuf.at[y], ydev(r))
    vb[0] = v_ref[...].T
    bb[z] = jnp.broadcast_to(b_ref[...].astype(F32) * LOG2E, (8, tb))
    vmail.start(1, vb.at[0], vb.at[1], right)
    vmail.start(2, vb.at[0], vb.at[2], left)
    for r in range(1, nz):
        mail.start(m_b + r, bb.at[z], bb.at[z], zdev(lax.rem(z + r, nz)))
    umail.start(1, uw_ref, up_slab(z, 0), right)
    umail.start(2, uw_ref, up_slab(z, 0), left)
    for r in range(1, ny):
        mail.start(m_d + r, dw_ref, down_slab(0), ydev(r))

    def pass_up(i, src):
        slab = up_slab(zof(i), 0)
        ymail.start(4 * i, slab if src is None else src, slab, ydev(1))
        if ny > 2:
            ymail.start(4 * i + 1, slab if src is None else src, slab, ydev(-1))

    def relay_up(i):
        if ny > 2:
            zz = zof(i)
            ymail.arrived(4 * i, up_slab(zz, -1), ydev(-1))
            ymail.start(4 * i + 2, up_slab(zz, -1, 0), up_slab(zz, -1, 0), ydev(1))
            ymail.arrived(4 * i + 1, up_slab(zz, 1), ydev(1))
            ymail.start(4 * i + 3, up_slab(zz, 1, 1), up_slab(zz, 1, 1), ydev(-1))

    def take_up(i):
        zz = zof(i)
        if ny > 2:
            ymail.arrived(4 * i + 2, up_slab(zz, -2, 0), ydev(-1))
            ymail.arrived(4 * i + 3, up_slab(zz, 2, 1), ydev(1))
        else:
            ymail.arrived(4 * i, up_slab(zz, -1), ydev(-1))

    pass_up(0, uw_ref)
    g_ow.start(ow_ref)
    g_res.start(res_ref)
    up_slab(z, 0)[...] = uw_ref[...]
    down_slab(0)[...] = dw_ref[...]

    qbuf[y] = q_ref[...]
    kb[0] = k_ref[...]
    ow_full[pl.ds(me * hd, hd), :] = ow_ref[...]
    res_full[:, pl.ds(pl.multiple_of(me * dw, dw), dw)] = res_ref[...]
    tri[...] = (iota((tb, tb), 0) > iota((tb, tb), 1)).astype(BF16)

    for r in range(1, ny):
        mail.arrived(m_q + r, qbuf.at[lax.rem(y + ny - r, ny)], ydev(r))
    for r in range(1, nz):
        mail.arrived(m_b + r, bb.at[lax.rem(z + nz - r, nz)], left)

    scale = hd ** (-0.5) * LOG2E
    hk = tb // 2
    ones = jnp.ones((8, tb), BF16)

    @pl.loop(0, nz)
    def _(i):
        odd = lax.rem(i, 2)
        zb = zof(i)
        onward = zdev(lax.rem(jnp.where(odd == 1, z + 1, z - 1) + nz, nz))

        @pl.when(i > 0)
        def _():
            kmail.arrived(i, kb.at[i], onward)
            vmail.arrived(i, vb.at[i], onward)

        @pl.when(jnp.logical_and(i >= 1, i <= nz - 4))
        def _():
            kmail.start(i + 2, kb.at[i], kb.at[i + 2], onward)
            vmail.start(i + 2, vb.at[i], vb.at[i + 2], onward)

        @pl.when(i == nz - 3)
        def _():
            kmail.start(nz - 1, kb.at[i], kb.at[nz - 1], onward)

        @pl.when(i == nz - 2)
        def _():
            vmail.start(nz - 1, vb.at[i], vb.at[nz - 1], onward)

        def tile(t, masked):
            def scored(h):
                q = qbuf[t, h * half : (h + 1) * half, :]
                scores = lax.dot_general(q, kb[i], NT, preferred_element_type=F32)
                logits = scores * scale + bb[zb][0:1, :]
                soft = jnp.maximum(
                    jnp.log(1.0 + jnp.exp2(jnp.minimum(logits, CLAMP))) * LOG2E, logits
                )
                brk = logits - soft
                if masked:
                    soft = jnp.where(strict(h), soft, 0.0)
                return brk, soft.astype(BF16)

            def strict(h):
                return iota((half, tb), 1) < iota((half, tb), 0) + h * half

            def weighed(h, brk, soft16):
                later0 = jnp.dot(soft16, tri[:, :hk], preferred_element_type=F32)
                later1 = jnp.dot(soft16[:, hk:], tri[hk:, hk:], preferred_element_type=F32)
                w0 = jnp.exp2(brk[:, :hk] - later0)
                w1 = jnp.exp2(brk[:, hk:] - later1)
                if masked:
                    w0 = jnp.where(strict(h)[:, :hk], w0, 0.0)
                    w1 = jnp.where(strict(h)[:, hk:], w1, 0.0)
                return w0.astype(BF16), w1.astype(BF16)

            def finish(h, soft16, w0, w1):
                where = pl.ds(pl.multiple_of(t * tb + h * half, half), half)
                pacc[zb, :, where] = lax.dot_general(
                    vb[i, :, :hk], w0, NT, preferred_element_type=F32
                ) + lax.dot_general(vb[i, :, hk:], w1, NT, preferred_element_type=F32)
                total = lax.dot_general(ones, soft16, NT, preferred_element_type=F32)
                tt[y, pl.ds(zb, 1), where] = total[0:1, :]

            both = [scored(h) for h in range(2)]
            weights = [weighed(h, *both[h]) for h in range(2)]
            for h in range(2):
                finish(h, both[h][1], *weights[h])

        @pl.loop(0, ny)
        def _(t):
            qblock = z * ny + t
            kblock = zb * ny + y

            @pl.when(kblock < qblock)
            def _():
                tile(t, False)

            @pl.when(kblock == qblock)
            def _():
                tile(t, True)

            @pl.when(kblock > qblock)
            def _():
                where = pl.ds(pl.multiple_of(t * tb, tb), tb)
                pacc[zb, :, where] = jnp.zeros((hd, tb), F32)
                tt[y, pl.ds(zb, 1), where] = jnp.zeros((1, tb), F32)

        @pl.when(jnp.logical_and(i > 0, i < nz - 1))
        def _():
            umail.arrived(i, up_slab(zb, 0), onward)

        @pl.when(jnp.logical_and(i >= 1, i <= nz - 4))
        def _():
            umail.start(i + 2, up_slab(zb, 0), up_slab(zb, 0), onward)

        @pl.when(i == nz - 3)
        def _():
            umail.start(nz - 1, up_slab(zb, 0, 0), up_slab(zb, 0, 0), onward)

        @pl.when(i == nz - 2)
        def _():
            umail.start(nz, up_slab(zb, 0, 1), up_slab(zb, 0, 1), onward)
            for r in range(1, ny):
                mail.arrived(m_d + r, down_slab(-r), ydev(r))
            for h in range(2):
                for j, to in ((1, right), (2, left)):
                    dmail.start(2 * j + h, down_half(z, h), down_half(z, h), to)

        @pl.when(jnp.logical_and(i > 0, i < nz - 1))
        def _():
            pass_up(i, None)

        @pl.when(i >= 2)
        def _():
            relay_up(i - 2)

    def down_tick(step, h):
        for i, to in ((2 * step - 1, right), (2 * step, left)):
            zz = zof(i)
            dmail.arrived(2 * i + h, down_half(zz, h), to)
            if i + 2 < nz - 1:
                dmail.start(2 * (i + 2) + h, down_half(zz, h), down_half(zz, h), to)
            elif (i + h) % 2 == 1:
                dmail.start(2 * (nz - 1) + h, down_half(zz, h), down_half(zz, h), to)

    final = nz // 2 - 1

    for r in range(1, ny):
        mail.start(m_t + r, tt.at[y], tt.at[y], ydev(r))
    last = zof(nz - 1)
    umail.arrived(nz - 1, up_slab(last, 0, 0), left)
    umail.arrived(nz, up_slab(last, 0, 1), right)
    pass_up(nz - 1, None)
    g_ow.forward()
    g_res.forward()
    for r in range(1, ny):
        mail.arrived(m_t + r, tt.at[lax.rem(y + ny - r, ny)], ydev(r))
    every = tt[0]
    after = jnp.zeros_like(every)
    for yy in range(ny):
        if yy:
            every = every + tt[yy]
        after = after + jnp.where(yy > y, tt[yy], 0.0)
    beyond = jnp.zeros_like(every[0:1, :])
    for zz in reversed(range(nz)):
        fac[zz : zz + 1, :] = jnp.exp2(-(beyond + after[zz : zz + 1, :]))
        beyond = beyond + every[zz : zz + 1, :]

    if final > 1:
        down_tick(1, 0)
    per = tb // 128

    @pl.loop(0, rows // 128)
    def _(n):
        at = pl.ds(pl.multiple_of(n * 128, 128), 128)
        acc = fac[0:1, at] * pacc[0, :, at]
        for zz in range(1, nz):
            acc = acc + fac[zz : zz + 1, at] * pacc[zz, :, at]
        col = pl.ds(pl.multiple_of(lax.rem(n, per) * 128, 128), 128)
        partf[n // per, :, col] = acc
        part[n // per, :, col] = acc.astype(BF16)

    for r in range(1, ny):
        mail.start(m_p + r, part.at[lax.rem(y + r, ny)], prec.at[y], ydev(r))
    relay_up(nz - 2)
    for r in range(1, ny):
        mail.arrived(m_p + r, prec.at[lax.rem(y + ny - r, ny)], ydev(r))
    mycol = pl.ds(pl.multiple_of(me * hd, hd), hd)
    for h in range(2):
        side = slice(h * half, (h + 1) * half)
        acc = partf[y, :, side]
        for r in range(1, ny):
            acc = acc + prec[lax.rem(y + r, ny), :, side].astype(F32)
        att_full[side, mycol] = acc.T.astype(BF16)
        g_att[h].start(att_full.at[pl.ds(h * half, half), mycol])
    relay_up(nz - 1)
    if final > 1:
        down_tick(1, 1)
    g_ow.finish()
    g_res.finish()
    g_att[0].forward()
    g_att[1].forward()
    if final > 2:
        down_tick(2, 0)
    g_att[0].finish()
    g_att[1].finish()

    width = ow_full.shape[1]
    nc = min(256, width)

    @pl.loop(0, width // nc)
    def _(n):
        at = pl.ds(pl.multiple_of(n * nc, nc), nc)
        pre[:, at] = jnp.dot(att_full[...], ow_full[:, at], preferred_element_type=F32) + (
            ALPHA * res_full[:, at].astype(F32)
        )

    if final > 2:
        down_tick(2, 1)
    rc = 64

    @pl.loop(0, tb // rc)
    def _(n):
        at = pl.ds(pl.multiple_of(n * rc, rc), rc)
        row = pre[at, :]
        center = jnp.mean(row, axis=-1, keepdims=True)
        off = row - center
        spread = jnp.mean(off * off, axis=-1, keepdims=True)
        fo_ref[at, :] = (off * lax.rsqrt(spread + EPSILON) * gain_ref[...] + shift_ref[...]).astype(
            BF16
        )

    for i in range(nz):
        take_up(i)
    hidden = up_full.shape[1]
    hc = min(256, hidden)

    @pl.loop(0, hidden // hc)
    def _(n):
        at = pl.ds(pl.multiple_of(n * hc, hc), hc)
        h = jnp.maximum(jnp.dot(fo_ref[...], up_full[:, at], preferred_element_type=F32), 0.0)
        act[:, at] = (h * h).astype(BF16)

    ntp = 2 * nx
    x, c = me // 2, lax.rem(me, 2)
    smail, xmail, tmail = Mail(ssend, srecv), Mail(xsend, xrecv), Mail(tsend, trecv)
    sibling = {"tp": x * 2 + 1 - c}
    fw = out_ref.shape[1]

    def mix(i):
        j = zof(i)
        chip = j // 2
        piece = lax.dot_general(
            act[...],
            down_full[pl.ds(pl.multiple_of(j * fw, fw), fw), :],
            NT,
            preferred_element_type=F32,
        )

        @pl.when(lax.rem(j, 2) != c)
        def _():
            sbuf[chip] = piece.astype(BF16)
            smail.start(chip, sbuf.at[chip], sib.at[chip], sibling)

        @pl.when(lax.rem(j, 2) == c)
        def _():
            hold[...] = piece

    def settle(i):
        j = zof(i)
        chip = j // 2

        @pl.when(lax.rem(j, 2) == c)
        def _():
            smail.arrived(chip, sib.at[chip], sibling)
            both = hold[...] + sib[chip].astype(F32)

            @pl.when(chip != x)
            def _():
                xbuf[chip] = both.astype(BF16)
                xmail.start(chip, xbuf.at[chip], rbuf.at[x], {"tp": j}, there=x)

            @pl.when(chip == x)
            def _():
                mine[...] = both

    down_tick(final, 0)

    @pl.loop(0, nz)
    def _(i):
        @pl.when(i == nz - 3)
        def _():
            down_tick(final, 1)

        @pl.when(i == nz - 1)
        def _():
            zz = zof(nz - 1)
            dmail.arrived(2 * (nz - 1), down_half(zz, 0), left)
            dmail.arrived(2 * (nz - 1) + 1, down_half(zz, 1), right)

        mix(i)
        settle(i)

    at = pl.ds(pl.multiple_of(me * fw, fw), fw)
    mine[...] = mine[...] + ALPHA * fo_ref[:, at].astype(F32)
    for r in range(1, nx):
        n = lax.rem(x + r, nx)
        xmail.arrived(n, rbuf.at[n], sibling)
        mine[...] = mine[...] + rbuf[n].astype(F32)
    total = mine[...]
    row_sum = jnp.sum(total, axis=-1, keepdims=True)
    row_squares = jnp.sum(total * total, axis=-1, keepdims=True)
    lane = iota((tb, 128), 1)
    cols[...] = jnp.where(lane == 0, row_sum, jnp.where(lane == 1, row_squares, 0.0))
    for n in range(tb // 128):
        stat[me, :, n * 128 : (n + 1) * 128] = cols[n * 128 : (n + 1) * 128, :].T[:8, :]
    for r in range(1, ntp):
        tmail.start(r, stat.at[me], stat.at[me], {"tp": lax.rem(me + r, ntp)})
    for r in range(1, ntp):
        tmail.arrived(r, stat.at[lax.rem(me + ntp - r, ntp)], sibling)
    sums = stat[0]
    for j in range(1, ntp):
        sums = sums + stat[j]
    d = float(fw * ntp)
    padded = jnp.concatenate([sums, jnp.zeros((120, tb), F32)], axis=0)
    for n in range(tb // 128):
        rows_n = slice(n * 128, (n + 1) * 128)
        both = padded[:, rows_n].T
        center = both[:, 0:1] / d
        spread = both[:, 1:2] / d - center * center
        out_ref[rows_n, :] = (
            (mine[rows_n, :] - center) * lax.rsqrt(spread + EPSILON) * gain2_ref[:, at]
            + shift2_ref[:, at]
        ).astype(BF16)

    for r in range(1, ny):
        mail.sent(m_q + r, q_ref, left)
        mail.sent(m_t + r, tt.at[y], left)
        mail.sent(m_p + r, prec.at[y], left)
    for r in range(1, nz):
        mail.sent(m_b + r, bb.at[z], left)
    for r in range(1, ny):
        mail.sent(m_d + r, dw_ref, left)
    for i in range(1, nz + 1):
        umail.sent(i, up_slab(0, 0) if i < nz - 1 else up_slab(0, 0, 0), left)
    for i in range(nz):
        ymail.sent(4 * i, up_slab(0, 0), left)
        if ny > 2:
            ymail.sent(4 * i + 1, up_slab(0, 0), left)
            ymail.sent(4 * i + 2, up_slab(0, 0, 0), left)
            ymail.sent(4 * i + 3, up_slab(0, 0, 0), left)
    for i in range(1, nz):
        for h in range(2):
            dmail.sent(2 * i + h, down_half(0, 0), left)
    for n in range(nx):
        smail.sent(n, sbuf.at[0], sibling)
    for r in range(1, nx):
        xmail.sent(lax.rem(x + r, nx), rbuf.at[0], sibling)
    for r in range(1, ntp):
        tmail.sent(r, stat.at[me], sibling)

    @pl.loop(1, nz)
    def _(i):
        kmail.sent(i, kb.at[0], left)
        vmail.sent(i, vb.at[0], left)

    for g in [g_ow, g_res] + g_att:
        g.drain()


def layer(nz, ny, nx, q, k, v, bias, ow, res, gain, shift, uw, dw, gain2, shift2):
    tb, hd = q.shape
    half = tb // 2
    rows = ny * tb
    width = ow.shape[1]
    ntp = 2 * nx
    fw = width // ntp
    hidden = uw.shape[1]
    messages = 4 * ny + nz + 4 * Gather.count(nx)
    vm = pl.BlockSpec(memory_space=pltpu.VMEM)
    dma = pltpu.SemaphoreType.DMA
    pairs = [messages, nz, nz, nz + 1, 4 * nz, 2 * nz, nx, nx, ntp]
    return pl.pallas_call(
        functools.partial(layer_kernel, nz, ny, nx),
        out_shape=jax.ShapeDtypeStruct((tb, fw), BF16),
        in_specs=[vm] * 12,
        out_specs=vm,
        scratch_shapes=[
            pltpu.VMEM((ny, tb, hd), BF16),
            pltpu.VMEM((nz, tb, hd), BF16),
            pltpu.VMEM((nz, hd, tb), BF16),
            pltpu.VMEM((nz, 8, tb), F32),
            pltpu.VMEM((tb, tb), BF16),
            pltpu.VMEM((nz, hd, rows), F32),
            pltpu.VMEM((ny, nz, rows), F32),
            pltpu.VMEM((nz, rows), F32),
            pltpu.VMEM((ny, hd, tb), BF16),
            pltpu.VMEM((ny, hd, tb), F32),
            pltpu.VMEM((ny, hd, tb), BF16),
            pltpu.VMEM((ntp * hd, width), BF16),
            pltpu.VMEM((tb, width), BF16),
            pltpu.VMEM((tb, ntp * hd), BF16),
            pltpu.VMEM((tb, width), F32),
            pltpu.VMEM((tb, width), BF16),
            pltpu.VMEM((width, hidden), BF16),
            pltpu.VMEM((width, hidden), BF16),
            pltpu.VMEM((tb, hidden), BF16),
            pltpu.VMEM((tb, fw), F32),
            pltpu.VMEM((nx, tb, fw), BF16),
            pltpu.VMEM((nx, tb, fw), BF16),
            pltpu.VMEM((nx, tb, fw), BF16),
            pltpu.VMEM((nx, tb, fw), BF16),
            pltpu.VMEM((tb, fw), F32),
            pltpu.VMEM((tb, 128), F32),
            pltpu.VMEM((ntp, 8, tb), F32),
        ]
        + [dma((n,)) for n in pairs for _ in range(2)],
        compiler_params=pltpu.CompilerParams(
            collective_id=0, has_side_effects=True, vmem_limit_bytes=60 * 1024 * 1024
        ),
        name="layer",
    )(q, k, v, bias, ow, res, gain, shift, uw, dw, gain2, shift2)


def body(nz, ny, nx, queries, keys, values, breaks, residual_in, out_weight, first_gain,
         first_shift, up_weight, down_weight, second_gain, second_shift):
    row = lambda a: a.reshape(1, -1)
    return layer(
        nz, ny, nx, queries, keys, values, row(breaks), out_weight, residual_in,
        row(first_gain), row(first_shift), up_weight, down_weight, row(second_gain), row(second_shift),
    )


def solution(mesh):
    nz, ny = split_sp(mesh.shape["sp"])
    nx = mesh.shape["tp"] // 2
    return jax.shard_map(
        functools.partial(body, nz, ny, nx),
        mesh=mesh,
        in_specs=(
            P("sp", "tp"),
            P("sp", "tp"),
            P("sp", "tp"),
            P("sp", "tp"),
            P("sp", "tp"),
            P("tp", None),
            P(),
            P(),
            P("sp", "tp"),
            P("sp", "tp"),
            P(),
            P(),
        ),
        out_specs=P("sp", "tp"),
        check_vma=False,
    )
```

```python
import functools
import math

import jax
import jax.numpy as jnp
from jax import lax
from jax.experimental import pallas as pl
from jax.experimental.pallas import tpu as pltpu
from jax.sharding import PartitionSpec as P

MESH = pl.DeviceIdType.MESH
ALPHA = 2.0**0.25
EPSILON = 1e-05
LOG2E = math.log2(math.e)
CLAMP = 120.0
F32 = jnp.float32
BF16 = jnp.bfloat16
NT = (((1,), (1,)), ((), ()))


def split_sp(n_sp):
    ny = 4 if n_sp >= 16 else 2
    return n_sp // ny, ny


def iota(shape, dim):
    return lax.broadcasted_iota(jnp.int32, shape, dim)


class Mail:
    def __init__(self, send, recv):
        self.send, self.recv = send, recv

    def make(self, m, src, dst, target, there=None):
        return pltpu.make_async_remote_copy(
            src_ref=src,
            dst_ref=dst,
            send_sem=self.send.at[m],
            recv_sem=self.recv.at[m if there is None else there],
            device_id=target,
            device_id_type=MESH,
        )

    def start(self, m, src, dst, target, there=None):
        self.make(m, src, dst, target, there).start()

    def arrived(self, m, dst, target):
        self.make(m, dst, dst, target).wait_recv()

    def sent(self, m, src, target):
        self.make(m, src, src, target).wait_send()


class Gather:
    def __init__(self, mail, base, slot, nx):
        self.mail, self.base, self.slot, self.nx = mail, base, slot, nx
        me = lax.axis_index("tp")
        self.me, self.x, self.c = me, me // 2, me % 2
        self.sib = {"tp": self.x * 2 + 1 - self.c}

    @staticmethod
    def count(nx):
        return 2 * nx

    def at(self, r, core):
        return lax.rem(self.x + self.nx + r, self.nx) * 2 + core

    def start(self, src):
        for r in range(1, self.nx):
            self.mail.start(self.base + r, src, self.slot(self.me), {"tp": self.at(r, self.c)})
        self.mail.start(self.base, src, self.slot(self.me), self.sib)

    def forward(self):
        for r in range(1, self.nx):
            got = self.slot(self.at(-r, self.c))
            self.mail.arrived(self.base + r, got, self.sib)
            self.mail.start(self.base + self.nx + r, got, got, self.sib)

    def finish(self):
        other = 1 - self.c
        self.mail.arrived(self.base, self.slot(self.at(0, other)), self.sib)
        for r in range(1, self.nx):
            self.mail.arrived(self.base + self.nx + r, self.slot(self.at(-r, other)), self.sib)

    def drain(self):
        for r in range(self.nx):
            self.mail.sent(self.base + r, self.slot(self.me), self.sib)
        for r in range(1, self.nx):
            self.mail.sent(self.base + self.nx + r, self.slot(self.me), self.sib)


def layer_kernel(
    nz, ny, nx,
    q_ref, k_ref, v_ref, b_ref, ow_ref, res_ref, gain_ref, shift_ref,
    uw_ref, dw_ref, gain2_ref, shift2_ref,
    out_ref,
    qbuf, kb, vb, bb, tri, pacc, tt, fac, part, partf, prec,
    ow_full, res_full, att_full, pre, fo_ref,
    up_full, down_full, act, sbuf, sib, xbuf, rbuf, mine, cols, stat,
    msend, mrecv, ksend, krecv, vsend, vrecv,
    usend, urecv, ysend, yrecv, dsend, drecv,
    ssend, srecv, xsend, xrecv, tsend, trecv,
):
    sp = lax.axis_index("sp")
    z, y = sp // ny, lax.rem(sp, ny)
    me = lax.axis_index("tp")
    tb, hd = k_ref.shape
    half = tb // 2
    rows = ny * tb
    mail = Mail(msend, mrecv)
    kmail, vmail = Mail(ksend, krecv), Mail(vsend, vrecv)
    umail, ymail, dmail = Mail(usend, urecv), Mail(ysend, yrecv), Mail(dsend, drecv)
    wr = uw_ref.shape[0]
    dw = res_ref.shape[1]

    def zdev(zz):
        return {"sp": zz * ny + y}

    def ydev(r):
        return {"sp": z * ny + lax.rem(y + ny + r, ny)}

    def zof(i):
        odd, step = lax.rem(i, 2), (i + 1) // 2
        return lax.rem(jnp.where(odd == 1, z - step, z + step) + nz, nz)

    def up_slab(zz, r, part=None):
        at = (zz * ny + lax.rem(y + ny + r, ny)) * wr
        n = wr if part is None else wr // 2
        return up_full.at[pl.ds(pl.multiple_of(at + (part or 0) * n, n), n), :]

    dh = ny * wr // 2

    def down_half(zz, h):
        return down_full.at[pl.ds(pl.multiple_of((zz * 2 + h) * dh, dh), dh), :]

    def down_slab(r):
        at = (z * ny + lax.rem(y + ny + r, ny)) * wr
        return down_full.at[pl.ds(pl.multiple_of(at, wr), wr), :]

    barrier = pltpu.get_barrier_semaphore()
    for r in range(1, nz):
        pl.semaphore_signal(barrier, inc=1, device_id=zdev(lax.rem(z + r, nz)), device_id_type=MESH)
    for r in range(1, ny):
        pl.semaphore_signal(barrier, inc=1, device_id=ydev(r), device_id_type=MESH)
    for r in range(1, 2 * nx):
        pl.semaphore_signal(
            barrier, inc=1, device_id={"tp": lax.rem(me + r, 2 * nx)}, device_id_type=MESH
        )
    vb[0] = v_ref[...].T
    bb[z] = jnp.broadcast_to(b_ref[...].astype(F32) * LOG2E, (8, tb))
    qbuf[y] = q_ref[...]
    kb[0] = k_ref[...]
    up_slab(z, 0)[...] = uw_ref[...]
    down_slab(0)[...] = dw_ref[...]
    ow_full[pl.ds(me * hd, hd), :] = ow_ref[...]
    res_full[:, pl.ds(pl.multiple_of(me * dw, dw), dw)] = res_ref[...]
    tri[...] = (iota((tb, tb), 0) > iota((tb, tb), 1)).astype(BF16)
    pl.semaphore_wait(barrier, nz - 1 + ny - 1 + 2 * nx - 1)

    m_q = 0
    m_b = ny
    m_t = m_b + nz
    m_p = m_t + ny
    m_d = m_p + 2 * ny
    g0 = m_d + ny
    gn = Gather.count(nx)
    g_ow = Gather(mail, g0, lambda j: ow_full.at[pl.ds(j * hd, hd), :], nx)
    g_res = Gather(
        mail, g0 + gn, lambda j: res_full.at[:, pl.ds(pl.multiple_of(j * dw, dw), dw)], nx
    )
    g_att = [
        Gather(
            mail,
            g0 + (2 + h) * gn,
            functools.partial(
                lambda h, j: att_full.at[pl.ds(h * half, half), pl.ds(pl.multiple_of(j * hd, hd), hd)], h
            ),
            nx,
        )
        for h in range(2)
    ]

    right, left = zdev(lax.rem(z + 1, nz)), zdev(lax.rem(z + nz - 1, nz))
    kmail.start(1, k_ref, kb.at[1], right)
    kmail.start(2, k_ref, kb.at[2], left)
    for r in range(1, ny):
        mail.start(m_q + r, q_ref, qbuf.at[y], ydev(r))
    vmail.start(1, vb.at[0], vb.at[1], right)
    vmail.start(2, vb.at[0], vb.at[2], left)
    for r in range(1, nz):
        mail.start(m_b + r, bb.at[z], bb.at[z], zdev(lax.rem(z + r, nz)))
    umail.start(1, uw_ref, up_slab(z, 0), right)
    umail.start(2, uw_ref, up_slab(z, 0), left)
    for r in range(1, ny):
        mail.start(m_d + r, dw_ref, down_slab(0), ydev(r))

    def pass_up(i, src):
        slab = up_slab(zof(i), 0)
        ymail.start(4 * i, slab if src is None else src, slab, ydev(1))
        if ny > 2:
            ymail.start(4 * i + 1, slab if src is None else src, slab, ydev(-1))

    def relay_up(i):
        if ny > 2:
            zz = zof(i)
            ymail.arrived(4 * i, up_slab(zz, -1), ydev(-1))
            ymail.start(4 * i + 2, up_slab(zz, -1, 0), up_slab(zz, -1, 0), ydev(1))
            ymail.arrived(4 * i + 1, up_slab(zz, 1), ydev(1))
            ymail.start(4 * i + 3, up_slab(zz, 1, 1), up_slab(zz, 1, 1), ydev(-1))

    def take_up(i):
        zz = zof(i)
        if ny > 2:
            ymail.arrived(4 * i + 2, up_slab(zz, -2, 0), ydev(-1))
            ymail.arrived(4 * i + 3, up_slab(zz, 2, 1), ydev(1))
        else:
            ymail.arrived(4 * i, up_slab(zz, -1), ydev(-1))

    pass_up(0, uw_ref)
    g_ow.start(ow_ref)
    g_res.start(res_ref)

    def onward(i):
        return zdev(lax.rem(jnp.where(lax.rem(i, 2) == 1, z + 1, z - 1) + nz, nz))

    def pass_keys(i):
        to = onward(i)
        kmail.arrived(i, kb.at[i], to)

        @pl.when(i <= nz - 4)
        def _():
            kmail.start(i + 2, kb.at[i], kb.at[i + 2], to)

        @pl.when(i == nz - 3)
        def _():
            kmail.start(nz - 1, kb.at[i], kb.at[nz - 1], to)

        vmail.arrived(i, vb.at[i], to)

        @pl.when(i <= nz - 4)
        def _():
            vmail.start(i + 2, vb.at[i], vb.at[i + 2], to)

        @pl.when(i == nz - 2)
        def _():
            vmail.start(nz - 1, vb.at[i], vb.at[nz - 1], to)

    def ring_up(i):
        to = onward(i)
        zz = zof(i)
        umail.arrived(i, up_slab(zz, 0), to)

        @pl.when(i <= nz - 4)
        def _():
            umail.start(i + 2, up_slab(zz, 0), up_slab(zz, 0), to)

        @pl.when(i == nz - 3)
        def _():
            umail.start(nz - 1, up_slab(zz, 0, 0), up_slab(zz, 0, 0), to)

        @pl.when(i == nz - 2)
        def _():
            umail.start(nz, up_slab(zz, 0, 1), up_slab(zz, 0, 1), to)

    for i in (1, 2):
        pass_keys(jnp.int32(i))
    for r in range(1, ny):
        mail.arrived(m_q + r, qbuf.at[lax.rem(y + ny - r, ny)], ydev(r))
    for r in range(1, nz):
        mail.arrived(m_b + r, bb.at[lax.rem(z + nz - r, nz)], left)

    scale = hd ** (-0.5) * LOG2E
    hk = tb // 2
    ones = jnp.ones((8, tb), BF16)

    @pl.loop(0, nz)
    def _(i):
        odd = lax.rem(i, 2)
        zb = zof(i)
        @pl.when(jnp.logical_and(odd == 1, i > 1))
        def _():
            pass_keys(i)

            @pl.when(i + 1 < nz)
            def _():
                pass_keys(i + 1)

        def tile(t, masked):
            def scored(h):
                q = qbuf[t, h * half : (h + 1) * half, :]
                scores = lax.dot_general(q, kb[i], NT, preferred_element_type=F32)
                logits = scores * scale + bb[zb][0:1, :]
                soft = jnp.maximum(
                    jnp.log(1.0 + jnp.exp2(jnp.minimum(logits, CLAMP))) * LOG2E, logits
                )
                brk = logits - soft
                if masked:
                    soft = jnp.where(strict(h), soft, 0.0)
                return brk, soft.astype(BF16)

            def strict(h):
                return iota((half, tb), 1) < iota((half, tb), 0) + h * half

            def weighed(h, brk, soft16):
                later0 = jnp.dot(soft16, tri[:, :hk], preferred_element_type=F32)
                later1 = jnp.dot(soft16[:, hk:], tri[hk:, hk:], preferred_element_type=F32)
                w0 = jnp.exp2(brk[:, :hk] - later0)
                w1 = jnp.exp2(brk[:, hk:] - later1)
                if masked:
                    w0 = jnp.where(strict(h)[:, :hk], w0, 0.0)
                    w1 = jnp.where(strict(h)[:, hk:], w1, 0.0)
                return w0.astype(BF16), w1.astype(BF16)

            def finish(h, soft16, w0, w1):
                where = pl.ds(pl.multiple_of(t * tb + h * half, half), half)
                pacc[zb, :, where] = lax.dot_general(
                    vb[i, :, :hk], w0, NT, preferred_element_type=F32
                ) + lax.dot_general(vb[i, :, hk:], w1, NT, preferred_element_type=F32)
                total = lax.dot_general(ones, soft16, NT, preferred_element_type=F32)
                tt[y, pl.ds(zb, 1), where] = total[0:1, :]

            return scored, weighed, finish

        def run(tiles):
            stage1, stage2 = {}, {}
            parts = [(fns, h) for fns in tiles for h in range(2)]
            for n in range(len(parts) + 2):
                if n < len(parts):
                    fns, h = parts[n]
                    stage1[n] = fns[0](h)
                if 0 <= n - 1 < len(parts):
                    fns, h = parts[n - 1]
                    stage2[n - 1] = fns[1](h, *stage1[n - 1])
                if 0 <= n - 2:
                    fns, h = parts[n - 2]
                    fns[2](h, stage1[n - 2][1], *stage2[n - 2])

        @pl.when(zb < z)
        def _():
            run([tile(t, False) for t in range(ny)])

        @pl.when(zb > z)
        def _():
            pacc[zb] = jnp.zeros((hd, rows), F32)
            tt[y, pl.ds(zb, 1), :] = jnp.zeros((1, rows), F32)

        @pl.when(zb == z)
        def _():
            @pl.loop(0, ny)
            def _(t):
                @pl.when(t > y)
                def _():
                    run([tile(t, False)])

                @pl.when(t == y)
                def _():
                    run([tile(t, True)])

                @pl.when(t < y)
                def _():
                    where = pl.ds(pl.multiple_of(t * tb, tb), tb)
                    pacc[zb, :, where] = jnp.zeros((hd, tb), F32)
                    tt[y, pl.ds(zb, 1), where] = jnp.zeros((1, tb), F32)

        @pl.when(jnp.logical_and(odd == 1, i < nz - 1))
        def _():
            for n in (i, i + 1):
                ring_up(n)
            for n in (i, i + 1):
                pass_up(n, None)

        @pl.when(i == nz - 3)
        def _():
            for r in range(1, ny):
                mail.arrived(m_d + r, down_slab(-r), ydev(r))
            for h in range(2):
                for j, to in ((1, right), (2, left)):
                    dmail.start(2 * j + h, down_half(z, h), down_half(z, h), to)

        @pl.when(i >= 2)
        def _():
            relay_up(i - 2)

    def down_tick(step, h):
        for i, to in ((2 * step - 1, right), (2 * step, left)):
            zz = zof(i)
            dmail.arrived(2 * i + h, down_half(zz, h), to)
            if i + 2 < nz - 1:
                dmail.start(2 * (i + 2) + h, down_half(zz, h), down_half(zz, h), to)
            elif (i + h) % 2 == 1:
                dmail.start(2 * (nz - 1) + h, down_half(zz, h), down_half(zz, h), to)

    final = nz // 2 - 1

    for r in range(1, ny):
        mail.start(m_t + r, tt.at[y], tt.at[y], ydev(r))
    g_ow.forward()
    g_res.forward()
    for r in range(1, ny):
        mail.arrived(m_t + r, tt.at[lax.rem(y + ny - r, ny)], ydev(r))
    every = tt[0]
    after = jnp.zeros_like(every)
    for yy in range(ny):
        if yy:
            every = every + tt[yy]
        after = after + jnp.where(yy > y, tt[yy], 0.0)
    beyond = jnp.zeros_like(every[0:1, :])
    for zz in reversed(range(nz)):
        fac[zz : zz + 1, :] = jnp.exp2(-(beyond + after[zz : zz + 1, :]))
        beyond = beyond + every[zz : zz + 1, :]

    if final > 1:
        down_tick(1, 0)
    per = half // 128 if half >= 128 else 1
    wc = min(128, half)

    for h in range(2):

        @pl.loop(0, ny * per)
        def _(n):
            to = n // per
            off = lax.rem(n, per) * wc
            at = pl.ds(pl.multiple_of(to * tb + h * half + off, wc), wc)
            acc = fac[0:1, at] * pacc[0, :, at]
            for zz in range(1, nz):
                acc = acc + fac[zz : zz + 1, at] * pacc[zz, :, at]
            col = pl.ds(pl.multiple_of(off, wc), wc)
            partf[h, to, :, col] = acc
            part[h, to, :, col] = acc.astype(BF16)

        for r in range(1, ny):
            mail.start(m_p + h * ny + r, part.at[h, lax.rem(y + r, ny)], prec.at[h, y], ydev(r))

    last = zof(nz - 1)
    umail.arrived(nz - 1, up_slab(last, 0, 0), left)
    umail.arrived(nz, up_slab(last, 0, 1), right)
    pass_up(nz - 1, None)
    mycol = pl.ds(pl.multiple_of(me * hd, hd), hd)
    for h in range(2):
        acc = partf[h, y]
        for r in range(1, ny):
            frm = lax.rem(y + ny - r, ny)
            mail.arrived(m_p + h * ny + r, prec.at[h, frm], ydev(r))
            acc = acc + prec[h, frm].astype(F32)
        att_full[h * half : (h + 1) * half, mycol] = acc.T.astype(BF16)
        g_att[h].start(att_full.at[pl.ds(h * half, half), mycol])
    relay_up(nz - 2)
    g_ow.finish()
    g_res.finish()
    if final > 1:
        down_tick(1, 1)
    g_att[0].forward()
    g_att[1].forward()
    relay_up(nz - 1)

    width = ow_full.shape[1]
    nc = min(256, width)
    rc = 64
    hidden = up_full.shape[1]
    hc = min(256, hidden)
    ntp = 2 * nx
    x, c = me // 2, lax.rem(me, 2)
    smail, xmail, tmail = Mail(ssend, srecv), Mail(xsend, xrecv), Mail(tsend, trecv)
    sibling = {"tp": x * 2 + 1 - c}
    fw = out_ref.shape[1]

    def project(h):
        side = slice(h * half, (h + 1) * half)

        @pl.loop(0, width // nc)
        def _(n):
            at = pl.ds(pl.multiple_of(n * nc, nc), nc)
            pre[side, at] = jnp.dot(
                att_full[side, :], ow_full[:, at], preferred_element_type=F32
            ) + ALPHA * res_full[side, at].astype(F32)

        @pl.loop(0, half // rc)
        def _(n):
            at = pl.ds(pl.multiple_of(h * half + n * rc, rc), rc)
            row = pre[at, :]
            center = jnp.mean(row, axis=-1, keepdims=True)
            off = row - center
            spread = jnp.mean(off * off, axis=-1, keepdims=True)
            fo_ref[at, :] = (
                off * lax.rsqrt(spread + EPSILON) * gain_ref[...] + shift_ref[...]
            ).astype(BF16)

    def lift(h):
        side = slice(h * half, (h + 1) * half)

        @pl.loop(0, hidden // hc)
        def _(n):
            at = pl.ds(pl.multiple_of(n * hc, hc), hc)
            up = jnp.maximum(
                jnp.dot(fo_ref[side, :], up_full[:, at], preferred_element_type=F32), 0.0
            )
            act[side, at] = (up * up).astype(BF16)

    def piece(j, h):
        return lax.dot_general(
            act[h * half : (h + 1) * half, :],
            down_full[pl.ds(pl.multiple_of(j * fw, fw), fw), :],
            NT,
            preferred_element_type=F32,
        )

    def mix(lo, hi, halves):
        @pl.loop(lo, hi)
        def _(i):
            j = zof(i)
            chip = j // 2

            @pl.when(lax.rem(j, 2) != c)
            def _():
                for h in halves:
                    sbuf[h, chip] = piece(j, h).astype(BF16)
                    m = 2 * chip + h
                    smail.start(m, sbuf.at[h, chip], sib.at[h, chip], sibling)

        @pl.loop(lo, hi)
        def _(i):
            j = zof(i)
            chip = j // 2

            @pl.when(lax.rem(j, 2) == c)
            def _():
                for h in halves:
                    own = piece(j, h)
                    m = 2 * chip + h
                    smail.arrived(m, sib.at[h, chip], sibling)
                    both = own + sib[h, chip].astype(F32)

                    @pl.when(chip != x)
                    def _():
                        xbuf[h, chip] = both.astype(BF16)
                        xmail.start(
                            m, xbuf.at[h, chip], rbuf.at[h, x], {"tp": j}, there=2 * x + h
                        )

                    @pl.when(chip == x)
                    def _():
                        mine[h * half : (h + 1) * half, :] = both

    early = nz - 3
    for h in range(2):
        g_att[h].finish()
        project(h)
        if h == 0:
            for i in range(nz):
                take_up(i)
            if final > 2:
                down_tick(2, 0)
        lift(h)
        if final > 2 and h == 0:
            down_tick(2, 1)
        mix(0, early, (h,))
    down_tick(final, 0)
    down_tick(final, 1)
    mix(early, nz - 1, (0, 1))
    zz = zof(nz - 1)
    dmail.arrived(2 * (nz - 1), down_half(zz, 0), left)
    dmail.arrived(2 * (nz - 1) + 1, down_half(zz, 1), right)
    mix(nz - 1, nz, (0, 1))

    at = pl.ds(pl.multiple_of(me * fw, fw), fw)
    mine[...] = mine[...] + ALPHA * fo_ref[:, at].astype(F32)
    for h in range(2):
        side = slice(h * half, (h + 1) * half)
        for r in range(1, nx):
            n = lax.rem(x + r, nx)
            xmail.arrived(2 * n + h, rbuf.at[h, n], sibling)
            mine[side, :] = mine[side, :] + rbuf[h, n].astype(F32)
    total = mine[...]
    row_sum = jnp.sum(total, axis=-1, keepdims=True)
    row_squares = jnp.sum(total * total, axis=-1, keepdims=True)
    lane = iota((tb, 128), 1)
    cols[...] = jnp.where(lane == 0, row_sum, jnp.where(lane == 1, row_squares, 0.0))
    for n in range(tb // 128):
        stat[me, :, n * 128 : (n + 1) * 128] = cols[n * 128 : (n + 1) * 128, :].T[:8, :]
    for r in range(1, ntp):
        tmail.start(r, stat.at[me], stat.at[me], {"tp": lax.rem(me + r, ntp)})
    for r in range(1, ntp):
        tmail.arrived(r, stat.at[lax.rem(me + ntp - r, ntp)], sibling)
    sums = stat[0]
    for j in range(1, ntp):
        sums = sums + stat[j]
    d = float(fw * ntp)
    padded = jnp.concatenate([sums, jnp.zeros((120, tb), F32)], axis=0)
    for n in range(tb // 128):
        rows_n = slice(n * 128, (n + 1) * 128)
        both = padded[:, rows_n].T
        center = both[:, 0:1] / d
        spread = both[:, 1:2] / d - center * center
        out_ref[rows_n, :] = (
            (mine[rows_n, :] - center) * lax.rsqrt(spread + EPSILON) * gain2_ref[:, at]
            + shift2_ref[:, at]
        ).astype(BF16)

    for r in range(1, ny):
        mail.sent(m_q + r, q_ref, left)
        mail.sent(m_t + r, tt.at[y], left)
        mail.sent(m_p + r, prec.at[0, y], left)
        mail.sent(m_p + ny + r, prec.at[0, y], left)
    for r in range(1, nz):
        mail.sent(m_b + r, bb.at[z], left)
    for r in range(1, ny):
        mail.sent(m_d + r, dw_ref, left)
    for i in range(1, nz + 1):
        umail.sent(i, up_slab(0, 0) if i < nz - 1 else up_slab(0, 0, 0), left)
    for i in range(nz):
        ymail.sent(4 * i, up_slab(0, 0), left)
        if ny > 2:
            ymail.sent(4 * i + 1, up_slab(0, 0), left)
            ymail.sent(4 * i + 2, up_slab(0, 0, 0), left)
            ymail.sent(4 * i + 3, up_slab(0, 0, 0), left)
    for i in range(1, nz):
        for h in range(2):
            dmail.sent(2 * i + h, down_half(0, 0), left)
    for n in range(2 * nx):
        smail.sent(n, sbuf.at[0, 0], sibling)
    for r in range(1, nx):
        for h in range(2):
            xmail.sent(2 * lax.rem(x + r, nx) + h, rbuf.at[0, 0], sibling)
    for r in range(1, ntp):
        tmail.sent(r, stat.at[me], sibling)

    @pl.loop(1, nz)
    def _(i):
        kmail.sent(i, kb.at[0], left)
        vmail.sent(i, vb.at[0], left)

    for g in [g_ow, g_res] + g_att:
        g.drain()


def layer(nz, ny, nx, q, k, v, bias, ow, res, gain, shift, uw, dw, gain2, shift2):
    tb, hd = q.shape
    half = tb // 2
    rows = ny * tb
    width = ow.shape[1]
    ntp = 2 * nx
    fw = width // ntp
    hidden = uw.shape[1]
    messages = 5 * ny + nz + 4 * Gather.count(nx)
    vm = pl.BlockSpec(memory_space=pltpu.VMEM)
    dma = pltpu.SemaphoreType.DMA
    pairs = [messages, nz, nz, nz + 1, 4 * nz, 2 * nz, 2 * nx, 2 * nx, ntp]
    return pl.pallas_call(
        functools.partial(layer_kernel, nz, ny, nx),
        out_shape=jax.ShapeDtypeStruct((tb, fw), BF16),
        in_specs=[vm] * 12,
        out_specs=vm,
        scratch_shapes=[
            pltpu.VMEM((ny, tb, hd), BF16),
            pltpu.VMEM((nz, tb, hd), BF16),
            pltpu.VMEM((nz, hd, tb), BF16),
            pltpu.VMEM((nz, 8, tb), F32),
            pltpu.VMEM((tb, tb), BF16),
            pltpu.VMEM((nz, hd, rows), F32),
            pltpu.VMEM((ny, nz, rows), F32),
            pltpu.VMEM((nz, rows), F32),
            pltpu.VMEM((2, ny, hd, half), BF16),
            pltpu.VMEM((2, ny, hd, half), F32),
            pltpu.VMEM((2, ny, hd, half), BF16),
            pltpu.VMEM((ntp * hd, width), BF16),
            pltpu.VMEM((tb, width), BF16),
            pltpu.VMEM((tb, ntp * hd), BF16),
            pltpu.VMEM((tb, width), F32),
            pltpu.VMEM((tb, width), BF16),
            pltpu.VMEM((width, hidden), BF16),
            pltpu.VMEM((width, hidden), BF16),
            pltpu.VMEM((tb, hidden), BF16),
            pltpu.VMEM((2, nx, half, fw), BF16),
            pltpu.VMEM((2, nx, half, fw), BF16),
            pltpu.VMEM((2, nx, half, fw), BF16),
            pltpu.VMEM((2, nx, half, fw), BF16),
            pltpu.VMEM((tb, fw), F32),
            pltpu.VMEM((tb, 128), F32),
            pltpu.VMEM((ntp, 8, tb), F32),
        ]
        + [dma((n,)) for n in pairs for _ in range(2)],
        compiler_params=pltpu.CompilerParams(
            collective_id=0, has_side_effects=True, vmem_limit_bytes=60 * 1024 * 1024
        ),
        name="layer",
    )(q, k, v, bias, ow, res, gain, shift, uw, dw, gain2, shift2)


def body(nz, ny, nx, queries, keys, values, breaks, residual_in, out_weight, first_gain,
         first_shift, up_weight, down_weight, second_gain, second_shift):
    row = lambda a: a.reshape(1, -1)
    return layer(
        nz, ny, nx, queries, keys, values, row(breaks), out_weight, residual_in,
        row(first_gain), row(first_shift), up_weight, down_weight, row(second_gain), row(second_shift),
    )


def solution(mesh):
    nz, ny = split_sp(mesh.shape["sp"])
    nx = mesh.shape["tp"] // 2
    return jax.shard_map(
        functools.partial(body, nz, ny, nx),
        mesh=mesh,
        in_specs=(
            P("sp", "tp"),
            P("sp", "tp"),
            P("sp", "tp"),
            P("sp", "tp"),
            P("sp", "tp"),
            P("tp", None),
            P(),
            P(),
            P("sp", "tp"),
            P("sp", "tp"),
            P(),
            P(),
        ),
        out_specs=P("sp", "tp"),
        check_vma=False,
    )
```

```python
import functools
import math

import jax
import jax.numpy as jnp
from jax import lax
from jax.experimental import pallas as pl
from jax.experimental.pallas import tpu as pltpu
from jax.sharding import PartitionSpec as P

MESH = pl.DeviceIdType.MESH
ALPHA = 2.0**0.25
EPSILON = 1e-05
LOG2E = math.log2(math.e)
CLAMP = 120.0
F32 = jnp.float32
BF16 = jnp.bfloat16
NT = (((1,), (1,)), ((), ()))


def split_sp(n_sp):
    ny = 4 if n_sp >= 16 else 2
    return n_sp // ny, ny


def iota(shape, dim):
    return lax.broadcasted_iota(jnp.int32, shape, dim)


class Mail:
    def __init__(self, send, recv):
        self.send, self.recv = send, recv

    def make(self, m, src, dst, target, there=None):
        return pltpu.make_async_remote_copy(
            src_ref=src,
            dst_ref=dst,
            send_sem=self.send.at[m],
            recv_sem=self.recv.at[m if there is None else there],
            device_id=target,
            device_id_type=MESH,
        )

    def start(self, m, src, dst, target, there=None):
        self.make(m, src, dst, target, there).start()

    def arrived(self, m, dst, target):
        self.make(m, dst, dst, target).wait_recv()

    def sent(self, m, src, target):
        self.make(m, src, src, target).wait_send()


class Gather:
    def __init__(self, mail, base, slot, nx):
        self.mail, self.base, self.slot, self.nx = mail, base, slot, nx
        me = lax.axis_index("tp")
        self.me, self.x, self.c = me, me // 2, me % 2
        self.sib = {"tp": self.x * 2 + 1 - self.c}

    @staticmethod
    def count(nx):
        return 2 * nx

    def at(self, r, core):
        return lax.rem(self.x + self.nx + r, self.nx) * 2 + core

    def start(self, src):
        for r in range(1, self.nx):
            self.mail.start(self.base + r, src, self.slot(self.me), {"tp": self.at(r, self.c)})
        self.mail.start(self.base, src, self.slot(self.me), self.sib)

    def forward(self):
        for r in range(1, self.nx):
            got = self.slot(self.at(-r, self.c))
            self.mail.arrived(self.base + r, got, self.sib)
            self.mail.start(self.base + self.nx + r, got, got, self.sib)

    def finish(self):
        other = 1 - self.c
        self.mail.arrived(self.base, self.slot(self.at(0, other)), self.sib)
        for r in range(1, self.nx):
            self.mail.arrived(self.base + self.nx + r, self.slot(self.at(-r, other)), self.sib)

    def drain(self):
        for r in range(self.nx):
            self.mail.sent(self.base + r, self.slot(self.me), self.sib)
        for r in range(1, self.nx):
            self.mail.sent(self.base + self.nx + r, self.slot(self.me), self.sib)


def layer_kernel(
    nz, ny, nx,
    q_ref, k_ref, v_ref, b_ref, ow_ref, res_ref, gain_ref, shift_ref,
    uw_ref, dw_ref, gain2_ref, shift2_ref,
    out_ref,
    qbuf, kb, vb, bb, tri, pacc, tt, fac, part, partf, prec,
    ow_full, res_full, att_full, pre, fo_ref,
    up_full, down_full, act, sbuf, sib, xbuf, rbuf, mine, cols, stat,
    msend, mrecv, ksend, krecv, vsend, vrecv,
    usend, urecv, ysend, yrecv, dsend, drecv,
    ssend, srecv, xsend, xrecv, tsend, trecv,
):
    sp = lax.axis_index("sp")
    z, y = sp // ny, lax.rem(sp, ny)
    me = lax.axis_index("tp")
    tb, hd = k_ref.shape
    half = tb // 2
    rows = ny * tb
    mail = Mail(msend, mrecv)
    kmail, vmail = Mail(ksend, krecv), Mail(vsend, vrecv)
    umail, ymail, dmail = Mail(usend, urecv), Mail(ysend, yrecv), Mail(dsend, drecv)
    wr = uw_ref.shape[0]
    dw = res_ref.shape[1]

    def zdev(zz):
        return {"sp": zz * ny + y}

    def ydev(r):
        return {"sp": z * ny + lax.rem(y + ny + r, ny)}

    def zof(i):
        odd, step = lax.rem(i, 2), (i + 1) // 2
        return lax.rem(jnp.where(odd == 1, z - step, z + step) + nz, nz)

    def up_slab(zz, r, part=None):
        at = (zz * ny + lax.rem(y + ny + r, ny)) * wr
        n = wr if part is None else wr // 2
        return up_full.at[pl.ds(pl.multiple_of(at + (part or 0) * n, n), n), :]

    def break_row(zz):
        return bb.at[zz, pl.ds(0, 1)]

    dh = ny * wr // 2

    def down_half(zz, h):
        return down_full.at[pl.ds(pl.multiple_of((zz * 2 + h) * dh, dh), dh), :]

    def down_slab(r):
        at = (z * ny + lax.rem(y + ny + r, ny)) * wr
        return down_full.at[pl.ds(pl.multiple_of(at, wr), wr), :]

    barrier = pltpu.get_barrier_semaphore()
    for r in range(1, nz):
        pl.semaphore_signal(barrier, inc=1, device_id=zdev(lax.rem(z + r, nz)), device_id_type=MESH)
    for r in range(1, ny):
        pl.semaphore_signal(barrier, inc=1, device_id=ydev(r), device_id_type=MESH)
    for r in range(1, 2 * nx):
        pl.semaphore_signal(
            barrier, inc=1, device_id={"tp": lax.rem(me + r, 2 * nx)}, device_id_type=MESH
        )
    vb[0] = v_ref[...].T
    bb[z] = jnp.broadcast_to(b_ref[...].astype(F32) * LOG2E, (8, tb))
    qbuf[y] = q_ref[...]
    kb[0] = k_ref[...]
    up_slab(z, 0)[...] = uw_ref[...]
    down_slab(0)[...] = dw_ref[...]
    ow_full[pl.ds(me * hd, hd), :] = ow_ref[...]
    res_full[:, pl.ds(pl.multiple_of(me * dw, dw), dw)] = res_ref[...]
    tri[...] = (iota((tb, tb), 0) > iota((tb, tb), 1)).astype(BF16)
    pl.semaphore_wait(barrier, nz - 1 + ny - 1 + 2 * nx - 1)

    m_q = 0
    m_b = ny
    m_t = m_b + nz
    m_p = m_t + ny
    m_d = m_p + 2 * ny
    g0 = m_d + ny
    gn = Gather.count(nx)
    g_ow = Gather(mail, g0, lambda j: ow_full.at[pl.ds(j * hd, hd), :], nx)
    g_res = Gather(
        mail, g0 + gn, lambda j: res_full.at[:, pl.ds(pl.multiple_of(j * dw, dw), dw)], nx
    )
    g_att = [
        Gather(
            mail,
            g0 + (2 + h) * gn,
            functools.partial(
                lambda h, j: att_full.at[pl.ds(h * half, half), pl.ds(pl.multiple_of(j * hd, hd), hd)], h
            ),
            nx,
        )
        for h in range(2)
    ]

    right, left = zdev(lax.rem(z + 1, nz)), zdev(lax.rem(z + nz - 1, nz))
    kmail.start(1, k_ref, kb.at[1], right)
    kmail.start(2, k_ref, kb.at[2], left)
    for r in range(1, ny):
        mail.start(m_q + r, q_ref, qbuf.at[y], ydev(r))
    vmail.start(1, vb.at[0], vb.at[1], right)
    vmail.start(2, vb.at[0], vb.at[2], left)
    for r in range(1, nz):
        mail.start(m_b + r, break_row(z), break_row(z), zdev(lax.rem(z + r, nz)))
    umail.start(1, uw_ref, up_slab(z, 0), right)
    umail.start(2, uw_ref, up_slab(z, 0), left)
    for r in range(1, ny):
        mail.start(m_d + r, dw_ref, down_slab(0), ydev(r))

    def pass_up(i, src):
        slab = up_slab(zof(i), 0)
        ymail.start(4 * i, slab if src is None else src, slab, ydev(1))
        if ny > 2:
            ymail.start(4 * i + 1, slab if src is None else src, slab, ydev(-1))

    def relay_up(i):
        if ny > 2:
            zz = zof(i)
            ymail.arrived(4 * i, up_slab(zz, -1), ydev(-1))
            ymail.start(4 * i + 2, up_slab(zz, -1, 0), up_slab(zz, -1, 0), ydev(1))
            ymail.arrived(4 * i + 1, up_slab(zz, 1), ydev(1))
            ymail.start(4 * i + 3, up_slab(zz, 1, 1), up_slab(zz, 1, 1), ydev(-1))

    def take_up(i):
        zz = zof(i)
        if ny > 2:
            ymail.arrived(4 * i + 2, up_slab(zz, -2, 0), ydev(-1))
            ymail.arrived(4 * i + 3, up_slab(zz, 2, 1), ydev(1))
        else:
            ymail.arrived(4 * i, up_slab(zz, -1), ydev(-1))

    pass_up(0, uw_ref)
    g_ow.start(ow_ref)
    g_res.start(res_ref)

    def onward(i):
        return zdev(lax.rem(jnp.where(lax.rem(i, 2) == 1, z + 1, z - 1) + nz, nz))

    def pass_keys(i):
        to = onward(i)
        kmail.arrived(i, kb.at[i], to)

        @pl.when(i <= nz - 4)
        def _():
            kmail.start(i + 2, kb.at[i], kb.at[i + 2], to)

        @pl.when(i == nz - 3)
        def _():
            kmail.start(nz - 1, kb.at[i], kb.at[nz - 1], to)

        vmail.arrived(i, vb.at[i], to)

        @pl.when(i <= nz - 4)
        def _():
            vmail.start(i + 2, vb.at[i], vb.at[i + 2], to)

        @pl.when(i == nz - 2)
        def _():
            vmail.start(nz - 1, vb.at[i], vb.at[nz - 1], to)

    def ring_up(i):
        to = onward(i)
        zz = zof(i)
        umail.arrived(i, up_slab(zz, 0), to)

        @pl.when(i <= nz - 4)
        def _():
            umail.start(i + 2, up_slab(zz, 0), up_slab(zz, 0), to)

        @pl.when(i == nz - 3)
        def _():
            umail.start(nz - 1, up_slab(zz, 0, 0), up_slab(zz, 0, 0), to)

        @pl.when(i == nz - 2)
        def _():
            umail.start(nz, up_slab(zz, 0, 1), up_slab(zz, 0, 1), to)

    for i in (1, 2):
        pass_keys(jnp.int32(i))
    for r in range(1, ny):
        mail.arrived(m_q + r, qbuf.at[lax.rem(y + ny - r, ny)], ydev(r))
    for r in range(1, nz):
        mail.arrived(m_b + r, break_row(lax.rem(z + nz - r, nz)), left)

    scale = hd ** (-0.5) * LOG2E
    hk = tb // 2
    ones = jnp.ones((8, tb), BF16)

    @pl.loop(0, nz)
    def _(i):
        odd = lax.rem(i, 2)
        zb = zof(i)
        @pl.when(jnp.logical_and(odd == 1, i > 1))
        def _():
            pass_keys(i)

            @pl.when(i + 1 < nz)
            def _():
                pass_keys(i + 1)

        def tile(t, masked):
            def scored(h):
                q = qbuf[t, h * half : (h + 1) * half, :]
                scores = lax.dot_general(q, kb[i], NT, preferred_element_type=F32)
                logits = scores * scale + bb[zb, 0:1, :]
                soft = jnp.maximum(
                    jnp.log(1.0 + jnp.exp2(jnp.minimum(logits, CLAMP))) * LOG2E, logits
                )
                brk = logits - soft
                if masked:
                    soft = jnp.where(strict(h), soft, 0.0)
                return brk, soft.astype(BF16)

            def strict(h):
                return iota((half, tb), 1) < iota((half, tb), 0) + h * half

            def weighed(h, brk, soft16):
                later0 = jnp.dot(soft16, tri[:, :hk], preferred_element_type=F32)
                later1 = jnp.dot(soft16[:, hk:], tri[hk:, hk:], preferred_element_type=F32)
                w0 = jnp.exp2(brk[:, :hk] - later0)
                w1 = jnp.exp2(brk[:, hk:] - later1)
                if masked:
                    w0 = jnp.where(strict(h)[:, :hk], w0, 0.0)
                    w1 = jnp.where(strict(h)[:, hk:], w1, 0.0)
                return w0.astype(BF16), w1.astype(BF16)

            def finish(h, soft16, w0, w1):
                where = pl.ds(pl.multiple_of(t * tb + h * half, half), half)
                pacc[zb, :, where] = lax.dot_general(
                    vb[i, :, :hk], w0, NT, preferred_element_type=F32
                ) + lax.dot_general(vb[i, :, hk:], w1, NT, preferred_element_type=F32)
                total = lax.dot_general(ones, soft16, NT, preferred_element_type=F32)
                tt[y, pl.ds(zb, 1), where] = total[0:1, :]

            return scored, weighed, finish

        def run(tiles):
            stage1, stage2 = {}, {}
            parts = [(fns, h) for fns in tiles for h in range(2)]
            for n in range(len(parts) + 2):
                if n < len(parts):
                    fns, h = parts[n]
                    stage1[n] = fns[0](h)
                if 0 <= n - 1 < len(parts):
                    fns, h = parts[n - 1]
                    stage2[n - 1] = fns[1](h, *stage1[n - 1])
                if 0 <= n - 2:
                    fns, h = parts[n - 2]
                    fns[2](h, stage1[n - 2][1], *stage2[n - 2])

        @pl.when(zb < z)
        def _():
            run([tile(t, False) for t in range(ny)])

        @pl.when(zb > z)
        def _():
            pacc[zb] = jnp.zeros((hd, rows), F32)
            tt[y, pl.ds(zb, 1), :] = jnp.zeros((1, rows), F32)

        @pl.when(zb == z)
        def _():
            @pl.loop(0, ny)
            def _(t):
                @pl.when(t > y)
                def _():
                    run([tile(t, False)])

                @pl.when(t == y)
                def _():
                    run([tile(t, True)])

                @pl.when(t < y)
                def _():
                    where = pl.ds(pl.multiple_of(t * tb, tb), tb)
                    pacc[zb, :, where] = jnp.zeros((hd, tb), F32)
                    tt[y, pl.ds(zb, 1), where] = jnp.zeros((1, tb), F32)

        @pl.when(jnp.logical_and(odd == 1, i < nz - 1))
        def _():
            for n in (i, i + 1):
                ring_up(n)
            for n in (i, i + 1):
                pass_up(n, None)

        @pl.when(i == nz - 3)
        def _():
            for r in range(1, ny):
                mail.arrived(m_d + r, down_slab(-r), ydev(r))
            for h in range(2):
                for j, to in ((1, right), (2, left)):
                    dmail.start(2 * j + h, down_half(z, h), down_half(z, h), to)

        @pl.when(i >= 2)
        def _():
            relay_up(i - 2)

    def down_tick(step, h):
        for i, to in ((2 * step - 1, right), (2 * step, left)):
            zz = zof(i)
            dmail.arrived(2 * i + h, down_half(zz, h), to)
            if i + 2 < nz - 1:
                dmail.start(2 * (i + 2) + h, down_half(zz, h), down_half(zz, h), to)
            elif (i + h) % 2 == 1:
                dmail.start(2 * (nz - 1) + h, down_half(zz, h), down_half(zz, h), to)

    final = nz // 2 - 1

    for r in range(1, ny):
        mail.start(m_t + r, tt.at[y], tt.at[y], ydev(r))
    g_ow.forward()
    g_res.forward()
    for r in range(1, ny):
        mail.arrived(m_t + r, tt.at[lax.rem(y + ny - r, ny)], ydev(r))
    every = tt[0]
    after = jnp.zeros_like(every)
    for yy in range(ny):
        if yy:
            every = every + tt[yy]
        after = after + jnp.where(yy > y, tt[yy], 0.0)
    beyond = jnp.zeros_like(every[0:1, :])
    for zz in reversed(range(nz)):
        fac[zz : zz + 1, :] = jnp.exp2(-(beyond + after[zz : zz + 1, :]))
        beyond = beyond + every[zz : zz + 1, :]

    if final > 1:
        down_tick(1, 0)
    per = half // 128 if half >= 128 else 1
    wc = min(128, half)

    for h in range(2):

        @pl.loop(0, ny * per)
        def _(n):
            to = n // per
            off = lax.rem(n, per) * wc
            at = pl.ds(pl.multiple_of(to * tb + h * half + off, wc), wc)
            acc = fac[0:1, at] * pacc[0, :, at]
            for zz in range(1, nz):
                acc = acc + fac[zz : zz + 1, at] * pacc[zz, :, at]
            col = pl.ds(pl.multiple_of(off, wc), wc)
            partf[h, to, :, col] = acc
            part[h, to, :, col] = acc.astype(BF16)

        for r in range(1, ny):
            mail.start(m_p + h * ny + r, part.at[h, lax.rem(y + r, ny)], prec.at[h, y], ydev(r))

    last = zof(nz - 1)
    umail.arrived(nz - 1, up_slab(last, 0, 0), left)
    umail.arrived(nz, up_slab(last, 0, 1), right)
    pass_up(nz - 1, None)
    mycol = pl.ds(pl.multiple_of(me * hd, hd), hd)
    for h in range(2):
        acc = partf[h, y]
        for r in range(1, ny):
            frm = lax.rem(y + ny - r, ny)
            mail.arrived(m_p + h * ny + r, prec.at[h, frm], ydev(r))
            acc = acc + prec[h, frm].astype(F32)
        att_full[h * half : (h + 1) * half, mycol] = acc.T.astype(BF16)
        g_att[h].start(att_full.at[pl.ds(h * half, half), mycol])
    relay_up(nz - 2)
    g_ow.finish()
    g_res.finish()
    if final > 1:
        down_tick(1, 1)
    g_att[0].forward()
    g_att[1].forward()
    relay_up(nz - 1)

    width = ow_full.shape[1]
    nc = min(256, width)
    rc = 64
    hidden = up_full.shape[1]
    hc = min(256, hidden)
    ntp = 2 * nx
    x, c = me // 2, lax.rem(me, 2)
    smail, xmail, tmail = Mail(ssend, srecv), Mail(xsend, xrecv), Mail(tsend, trecv)
    sibling = {"tp": x * 2 + 1 - c}
    fw = out_ref.shape[1]

    def project(h):
        side = slice(h * half, (h + 1) * half)

        @pl.loop(0, width // nc)
        def _(n):
            at = pl.ds(pl.multiple_of(n * nc, nc), nc)
            pre[side, at] = jnp.dot(
                att_full[side, :], ow_full[:, at], preferred_element_type=F32
            ) + ALPHA * res_full[side, at].astype(F32)

        @pl.loop(0, half // rc)
        def _(n):
            at = pl.ds(pl.multiple_of(h * half + n * rc, rc), rc)
            row = pre[at, :]
            center = jnp.mean(row, axis=-1, keepdims=True)
            off = row - center
            spread = jnp.mean(off * off, axis=-1, keepdims=True)
            fo_ref[at, :] = (
                off * lax.rsqrt(spread + EPSILON) * gain_ref[...] + shift_ref[...]
            ).astype(BF16)

    def lift(h):
        side = slice(h * half, (h + 1) * half)

        @pl.loop(0, hidden // hc)
        def _(n):
            at = pl.ds(pl.multiple_of(n * hc, hc), hc)
            up = jnp.maximum(
                jnp.dot(fo_ref[side, :], up_full[:, at], preferred_element_type=F32), 0.0
            )
            act[side, at] = (up * up).astype(BF16)

    def piece(j, h):
        return lax.dot_general(
            act[h * half : (h + 1) * half, :],
            down_full[pl.ds(pl.multiple_of(j * fw, fw), fw), :],
            NT,
            preferred_element_type=F32,
        )

    def mix(lo, hi, halves):
        @pl.loop(lo, hi)
        def _(i):
            j = zof(i)
            chip = j // 2

            @pl.when(lax.rem(j, 2) != c)
            def _():
                for h in halves:
                    sbuf[h, chip] = piece(j, h).astype(BF16)
                    m = 2 * chip + h
                    smail.start(m, sbuf.at[h, chip], sib.at[h, chip], sibling)

        @pl.loop(lo, hi)
        def _(i):
            j = zof(i)
            chip = j // 2

            @pl.when(lax.rem(j, 2) == c)
            def _():
                for h in halves:
                    own = piece(j, h)
                    m = 2 * chip + h
                    smail.arrived(m, sib.at[h, chip], sibling)
                    both = own + sib[h, chip].astype(F32)

                    @pl.when(chip != x)
                    def _():
                        xbuf[h, chip] = both.astype(BF16)
                        xmail.start(
                            m, xbuf.at[h, chip], rbuf.at[h, x], {"tp": j}, there=2 * x + h
                        )

                    @pl.when(chip == x)
                    def _():
                        mine[h * half : (h + 1) * half, :] = both

    early = nz - 3
    for h in range(2):
        g_att[h].finish()
        project(h)
        if h == 0:
            for i in range(nz):
                take_up(i)
            if final > 2:
                down_tick(2, 0)
        lift(h)
        if final > 2 and h == 0:
            down_tick(2, 1)
        mix(0, early, (h,))
    down_tick(final, 0)
    down_tick(final, 1)
    mix(early, nz - 1, (0, 1))
    zz = zof(nz - 1)
    dmail.arrived(2 * (nz - 1), down_half(zz, 0), left)
    dmail.arrived(2 * (nz - 1) + 1, down_half(zz, 1), right)
    mix(nz - 1, nz, (0, 1))

    at = pl.ds(pl.multiple_of(me * fw, fw), fw)
    mine[...] = mine[...] + ALPHA * fo_ref[:, at].astype(F32)
    for h in range(2):
        side = slice(h * half, (h + 1) * half)
        for r in range(1, nx):
            n = lax.rem(x + r, nx)
            xmail.arrived(2 * n + h, rbuf.at[h, n], sibling)
            mine[side, :] = mine[side, :] + rbuf[h, n].astype(F32)
    total = mine[...]
    row_sum = jnp.sum(total, axis=-1, keepdims=True)
    row_squares = jnp.sum(total * total, axis=-1, keepdims=True)
    lane = iota((tb, 128), 1)
    cols[...] = jnp.where(lane == 0, row_sum, jnp.where(lane == 1, row_squares, 0.0))
    for n in range(tb // 128):
        stat[me, :, n * 128 : (n + 1) * 128] = cols[n * 128 : (n + 1) * 128, :].T[:8, :]
    for r in range(1, ntp):
        tmail.start(r, stat.at[me], stat.at[me], {"tp": lax.rem(me + r, ntp)})
    for r in range(1, ntp):
        tmail.arrived(r, stat.at[lax.rem(me + ntp - r, ntp)], sibling)
    sums = stat[0]
    for j in range(1, ntp):
        sums = sums + stat[j]
    d = float(fw * ntp)
    padded = jnp.concatenate([sums, jnp.zeros((120, tb), F32)], axis=0)
    for n in range(tb // 128):
        rows_n = slice(n * 128, (n + 1) * 128)
        both = padded[:, rows_n].T
        center = both[:, 0:1] / d
        spread = both[:, 1:2] / d - center * center
        out_ref[rows_n, :] = (
            (mine[rows_n, :] - center) * lax.rsqrt(spread + EPSILON) * gain2_ref[:, at]
            + shift2_ref[:, at]
        ).astype(BF16)

    for r in range(1, ny):
        mail.sent(m_q + r, q_ref, left)
        mail.sent(m_t + r, tt.at[y], left)
        mail.sent(m_p + r, prec.at[0, y], left)
        mail.sent(m_p + ny + r, prec.at[0, y], left)
    for r in range(1, nz):
        mail.sent(m_b + r, break_row(z), left)
    for r in range(1, ny):
        mail.sent(m_d + r, dw_ref, left)
    for i in range(1, nz + 1):
        umail.sent(i, up_slab(0, 0) if i < nz - 1 else up_slab(0, 0, 0), left)
    for i in range(nz):
        ymail.sent(4 * i, up_slab(0, 0), left)
        if ny > 2:
            ymail.sent(4 * i + 1, up_slab(0, 0), left)
            ymail.sent(4 * i + 2, up_slab(0, 0, 0), left)
            ymail.sent(4 * i + 3, up_slab(0, 0, 0), left)
    for i in range(1, nz):
        for h in range(2):
            dmail.sent(2 * i + h, down_half(0, 0), left)
    for n in range(2 * nx):
        smail.sent(n, sbuf.at[0, 0], sibling)
    for r in range(1, nx):
        for h in range(2):
            xmail.sent(2 * lax.rem(x + r, nx) + h, rbuf.at[0, 0], sibling)
    for r in range(1, ntp):
        tmail.sent(r, stat.at[me], sibling)

    @pl.loop(1, nz)
    def _(i):
        kmail.sent(i, kb.at[0], left)
        vmail.sent(i, vb.at[0], left)

    for g in [g_ow, g_res] + g_att:
        g.drain()


def layer(nz, ny, nx, q, k, v, bias, ow, res, gain, shift, uw, dw, gain2, shift2):
    tb, hd = q.shape
    half = tb // 2
    rows = ny * tb
    width = ow.shape[1]
    ntp = 2 * nx
    fw = width // ntp
    hidden = uw.shape[1]
    messages = 5 * ny + nz + 4 * Gather.count(nx)
    vm = pl.BlockSpec(memory_space=pltpu.VMEM)
    dma = pltpu.SemaphoreType.DMA
    pairs = [messages, nz, nz, nz + 1, 4 * nz, 2 * nz, 2 * nx, 2 * nx, ntp]
    return pl.pallas_call(
        functools.partial(layer_kernel, nz, ny, nx),
        out_shape=jax.ShapeDtypeStruct((tb, fw), BF16),
        in_specs=[vm] * 12,
        out_specs=vm,
        scratch_shapes=[
            pltpu.VMEM((ny, tb, hd), BF16),
            pltpu.VMEM((nz, tb, hd), BF16),
            pltpu.VMEM((nz, hd, tb), BF16),
            pltpu.VMEM((nz, 8, tb), F32),
            pltpu.VMEM((tb, tb), BF16),
            pltpu.VMEM((nz, hd, rows), F32),
            pltpu.VMEM((ny, nz, rows), F32),
            pltpu.VMEM((nz, rows), F32),
            pltpu.VMEM((2, ny, hd, half), BF16),
            pltpu.VMEM((2, ny, hd, half), F32),
            pltpu.VMEM((2, ny, hd, half), BF16),
            pltpu.VMEM((ntp * hd, width), BF16),
            pltpu.VMEM((tb, width), BF16),
            pltpu.VMEM((tb, ntp * hd), BF16),
            pltpu.VMEM((tb, width), F32),
            pltpu.VMEM((tb, width), BF16),
            pltpu.VMEM((width, hidden), BF16),
            pltpu.VMEM((width, hidden), BF16),
            pltpu.VMEM((tb, hidden), BF16),
            pltpu.VMEM((2, nx, half, fw), BF16),
            pltpu.VMEM((2, nx, half, fw), BF16),
            pltpu.VMEM((2, nx, half, fw), BF16),
            pltpu.VMEM((2, nx, half, fw), BF16),
            pltpu.VMEM((tb, fw), F32),
            pltpu.VMEM((tb, 128), F32),
            pltpu.VMEM((ntp, 8, tb), F32),
        ]
        + [dma((n,)) for n in pairs for _ in range(2)],
        compiler_params=pltpu.CompilerParams(
            collective_id=0, has_side_effects=True, vmem_limit_bytes=60 * 1024 * 1024
        ),
        name="layer",
    )(q, k, v, bias, ow, res, gain, shift, uw, dw, gain2, shift2)


def body(nz, ny, nx, queries, keys, values, breaks, residual_in, out_weight, first_gain,
         first_shift, up_weight, down_weight, second_gain, second_shift):
    row = lambda a: a.reshape(1, -1)
    return layer(
        nz, ny, nx, queries, keys, values, row(breaks), out_weight, residual_in,
        row(first_gain), row(first_shift), up_weight, down_weight, row(second_gain), row(second_shift),
    )


def solution(mesh):
    nz, ny = split_sp(mesh.shape["sp"])
    nx = mesh.shape["tp"] // 2
    return jax.shard_map(
        functools.partial(body, nz, ny, nx),
        mesh=mesh,
        in_specs=(
            P("sp", "tp"),
            P("sp", "tp"),
            P("sp", "tp"),
            P("sp", "tp"),
            P("sp", "tp"),
            P("tp", None),
            P(),
            P(),
            P("sp", "tp"),
            P("sp", "tp"),
            P(),
            P(),
        ),
        out_specs=P("sp", "tp"),
        check_vma=False,
    )
```
